32 devices in a mesh: sp: 8 (over z, y), tp: 4 (over x, core).
Axes of the slice: x: 2, y: 2, z: 4, core: 2. Of those that a mesh axis runs over, the one named last changes fastest.
Arguments:
- layer_input: bfloat16 [6144, 2048], P('sp', 'tp'), may hold values from -6 to 6
- input_norm_gain: bfloat16 [2048], replicated, may hold values from 0.099609375 to 1.8984375
- query_weight: bfloat16 [2048, 2048], P(None, 'tp'), may hold values from -0.125 to 0.125
- forget_weight: bfloat16 [2048, 2048], P(None, 'tp'), may hold values from -0.125 to 0.125
- value_matrix: bfloat16 [2048, 2048], P(None, 'tp'), may hold values from -0.125 to 0.125
- output_gate_weight: bfloat16 [2048, 2048], P(None, 'tp'), may hold values from -0.125 to 0.125
- after_gate_weight: bfloat16 [2048, 2048], P(None, 'tp'), may hold values from -0.125 to 0.125
- before_gate_weight: bfloat16 [2048, 2048], P(None, 'tp'), may hold values from -0.125 to 0.125
- convolution_input_weight: bfloat16 [2048, 2048], P(None, 'tp'), may hold values from -0.125 to 0.125
- forget_minimum: float32 [2048], P('tp'), may hold values from 0.95 to 0.9999837
- surge_log_decay: float32 [6144, 2048], P('sp', 'tp'), may hold values from -2.2 to 0
- convolution_kernel: bfloat16 [3, 2048], P(None, 'tp'), may hold values from -4 to 4
- head_norm_gain: bfloat16 [128], replicated, may hold values from 0.099609375 to 1.8984375
- starting_state: float32 [16, 128, 128], P('tp', 'sp'), may hold values from -0.09375 to 0.09375
- recurrence_output_weight: bfloat16 [2048, 2048], P('tp'), may hold values from -0.09375 to 0.09375
- convolution_output_weight: bfloat16 [2048, 2048], P('tp'), may hold values from -0.09375 to 0.09375
- output_norm_gain: bfloat16 [2048], replicated, may hold values from 0.099609375 to 1.8984375
Outputs:
- layer_out: bfloat16 [6144, 2048], P(('sp', 'tp'))
The draws below stay inside these ranges and needn't reach their ends.
All inputs are finite; a program needn't handle non-finite values.
Results may differ from the reference program's by a relative error of at most 0.014.
Values may be sent and summed in bfloat16 or wider, within the bound.
A program may use at most 128 MiB of HBM per device.

```python
import jax
import jax.numpy as jnp
from jax import lax

D = 2048
HEADS = 16
DK = 128
DV = 128
CW = 2048
CK = 3
BLK = 64
TOKENS_PER_SHARD = 768
TOKENS = 6144
KEYW = 2048
VALW = 2048


def decay_tables(key):
    keys = jax.random.split(jax.random.fold_in(key, 11), 6)
    share = 0.5
    slow_head = jax.random.uniform(keys[0], (HEADS,), jnp.float32) < share
    slow = jnp.repeat(slow_head, DK)
    rate = jnp.exp(jax.random.uniform(keys[1], (HEADS * DK,), jnp.float32, jnp.log(0.1), jnp.log(0.6))) / TOKENS
    fast_floor = jax.random.uniform(keys[2], (HEADS * DK,), jnp.float32, 0.95, 0.99)
    forget_minimum = jnp.where(slow, 1.0 - rate, fast_floor)
    extra_decay = jnp.where(slow, rate, 0.03)
    decay_factor = jnp.exp(jax.random.uniform(keys[3], (TOKENS // TOKENS_PER_SHARD,), jnp.float32, jnp.log(0.5), jnp.log(2.0)))
    spots = jax.random.randint(keys[4], (3,), 0, TOKENS)
    losses = jnp.log(jax.random.uniform(keys[5], (3,), jnp.float32, 0.5, 0.8))
    position = jnp.arange(TOKENS)
    decay_surge = jnp.sum(jnp.where(position[:, None] == spots[None, :], losses[None, :], 0.0), axis=1)
    surge_log_decay = -jnp.repeat(decay_factor, TOKENS_PER_SHARD)[:, None] * extra_decay[None, :] + decay_surge[:, None]
    return (forget_minimum.astype(jnp.float32), surge_log_decay.astype(jnp.float32))


def draw_forget_minimum(key, part):
    return decay_tables(key)[0]


def draw_surge_log_decay(key, part):
    return decay_tables(key)[1]


def shard_levels(key, shape, pieces, least, largest):
    factor_of, own = 1.0, jax.random.fold_in(key, 6)
    for dim, blocks in pieces:
        draws = jnp.exp(jax.random.uniform(jax.random.fold_in(own, dim), (blocks,), jnp.float32, least / len(pieces), largest / len(pieces)))
        factor_of = factor_of * jnp.repeat(draws, shape[dim] // blocks).reshape([-1 if axis == dim else 1 for axis in range(len(shape))])
    return factor_of


def normal_values(key, dims, deviation, limit, cuts=(), held_as=jnp.bfloat16):
    entries = jax.random.normal(key, dims, jnp.float32) * deviation
    if len(cuts) > 0:
        entries = shard_levels(key, dims, cuts, -0.22, 0.18) * entries
    return jnp.clip(entries, min=-limit, max=limit).astype(held_as)


def setup_inputs(seed: int = 0) -> dict:
    key_list = jax.random.split(jax.random.key(seed), 18)
    return {
        "layer_input": normal_values(key_list[0], (TOKENS, D), 1.0, 6.0, ((0, 8), (1, 4))),
        "input_norm_gain": jnp.clip(1.0 + 0.18 * jax.random.normal(key_list[1], (D,), jnp.float32), 0.099609375, 1.8984375).astype(jnp.bfloat16),
        "query_weight": normal_values(key_list[2], (D, KEYW), D ** -0.5, 0.125, ((1, 4),)),
        "forget_weight": normal_values(key_list[3], (D, KEYW), D ** -0.5, 0.125, ((1, 4),)),
        "value_matrix": normal_values(key_list[4], (D, VALW), D ** -0.5, 0.125, ((1, 4),)),
        "output_gate_weight": normal_values(key_list[5], (D, VALW), D ** -0.5, 0.125, ((1, 4),)),
        "after_gate_weight": normal_values(key_list[6], (D, CW), D ** -0.5, 0.125, ((1, 4),)),
        "before_gate_weight": normal_values(key_list[7], (D, CW), D ** -0.5, 0.125, ((1, 4),)),
        "convolution_input_weight": normal_values(key_list[8], (D, CW), D ** -0.5, 0.125, ((1, 4),)),
        "forget_minimum": draw_forget_minimum(jax.random.fold_in(key_list[17], 71), 0),
        "surge_log_decay": draw_surge_log_decay(jax.random.fold_in(key_list[17], 71), 0),
        "convolution_kernel": normal_values(key_list[11], (CK, CW), 0.577, 4.0, ((1, 4),)),
        "head_norm_gain": jnp.clip(1.0 + 0.18 * jax.random.normal(key_list[12], (DV,), jnp.float32), 0.099609375, 1.8984375).astype(jnp.bfloat16),
        "starting_state": normal_values(key_list[13], (HEADS, DK, DV), (0.5 * TOKENS ** -0.5), 0.09375, ((0, 4), (1, 8)), jnp.float32),
        "recurrence_output_weight": normal_values(key_list[14], (VALW, D), (VALW + CW) ** -0.5, 0.09375, ((0, 4),)),
        "convolution_output_weight": normal_values(key_list[15], (CW, D), (VALW + CW) ** -0.5, 0.09375, ((0, 4),)),
        "output_norm_gain": jnp.clip(1.0 + 0.18 * jax.random.normal(key_list[16], (D,), jnp.float32), 0.099609375, 1.8984375).astype(jnp.bfloat16),
    }


EPS = 1e-06
PRECISE_PRODUCT = lax.Precision.HIGHEST

def rms_scale(value_rows):
    return lax.rsqrt(lax.optimization_barrier(jnp.mean(value_rows * value_rows, axis=-1, keepdims=True)) + EPS)

def project(normed, weight):
    return jnp.dot(normed, weight, preferred_element_type=jnp.float32).astype(jnp.bfloat16)

def block_pass(latent_state, inputs):
    query_rows, key_inputs, value_rows, forget_gate_logits = inputs
    cumulative_decay = jnp.cumsum(forget_gate_logits, axis=1)
    length = query_rows.shape[1]
    causal_masking = jnp.tril(jnp.ones((length, length), dtype=bool))[None, :, :, None]
    crossed_output = jnp.einsum('rmq,rqu->rmu', query_rows * jnp.exp(cumulative_decay), latent_state, precision=PRECISE_PRODUCT)
    decay = jnp.exp(jnp.where(causal_masking, cumulative_decay[:, :, None, :] - cumulative_decay[:, None, :, :], -jnp.inf))
    scores = jnp.einsum('htk,hsk,htsk->hts', query_rows, key_inputs, decay, precision=PRECISE_PRODUCT)
    o_intra = jnp.einsum('hts,hsv->htv', scores, value_rows, precision=PRECISE_PRODUCT)
    final_state = cumulative_decay[:, -1:, :]
    latent_state = jnp.exp(final_state[:, 0, :])[..., None] * latent_state + jnp.einsum('xar,xai->xri', key_inputs * jnp.exp(final_state - cumulative_decay), value_rows, precision=PRECISE_PRODUCT)
    return (latent_state, o_intra + crossed_output)

def reference(layer_input, input_norm_gain, query_weight, forget_weight, value_matrix, output_gate_weight, after_gate_weight, before_gate_weight, convolution_input_weight, forget_minimum, surge_log_decay, convolution_kernel, head_norm_gain, starting_state, recurrence_output_weight, convolution_output_weight, output_norm_gain):
    rows_f = layer_input.astype(jnp.float32)
    normed = (rows_f * rms_scale(rows_f) * input_norm_gain.astype(jnp.float32)).astype(jnp.bfloat16)
    query_raw = project(normed, query_weight)
    forget_raw = project(normed, forget_weight)
    value_raw = project(normed, value_matrix)
    outgate_raw = project(normed, output_gate_weight)
    postgate_raw = project(normed, after_gate_weight)
    pregate_raw = project(normed, before_gate_weight)
    convval_raw = project(normed, convolution_input_weight)
    forget_single = forget_raw.astype(jnp.float32)
    forget_gate_logits = jnp.logaddexp(jnp.log(forget_minimum), jnp.log1p(-forget_minimum) + jax.nn.log_sigmoid(forget_single)) + surge_log_decay
    key_inputs = (1.0 - forget_minimum) * jax.nn.sigmoid(-forget_single)
    query_rows = jax.nn.silu(query_raw.astype(jnp.float32)) * DK ** (-0.5)
    blocks = TOKENS // BLK

    def to_blocks(value_rows, width):
        return value_rows.reshape(blocks, BLK, HEADS, width).transpose(0, 2, 1, 3)
    _, outputs = lax.scan(block_pass, starting_state.astype(jnp.float32), (to_blocks(query_rows, DK), to_blocks(key_inputs, DK), to_blocks(value_raw.astype(jnp.float32), DV), to_blocks(forget_gate_logits, DK)))
    recurrence_step = outputs.transpose(0, 2, 1, 3).reshape(TOKENS, HEADS, DV)
    normed_heads = recurrence_step * rms_scale(recurrence_step) * head_norm_gain.astype(jnp.float32)
    rec_out = (normed_heads.reshape(TOKENS, HEADS * DV) * jax.nn.silu(outgate_raw.astype(jnp.float32))).astype(jnp.bfloat16)
    mixed_in = pregate_raw.astype(jnp.float32) * convval_raw.astype(jnp.float32)
    padded = jnp.concatenate([jnp.zeros((CK - 1, mixed_in.shape[1]), jnp.float32), mixed_in], axis=0)
    taps_f = convolution_kernel.astype(jnp.float32)
    conv_sum = padded[0:TOKENS] * taps_f[0]
    for offset in range(1, CK):
        conv_sum = conv_sum + padded[offset:offset + TOKENS] * taps_f[offset]
    conv_out = (postgate_raw.astype(jnp.float32) * conv_sum).astype(jnp.bfloat16)
    mixed = jnp.dot(rec_out, recurrence_output_weight, preferred_element_type=jnp.float32) + jnp.dot(conv_out, convolution_output_weight, preferred_element_type=jnp.float32)
    return (mixed * rms_scale(mixed) * output_norm_gain.astype(jnp.float32)).astype(jnp.bfloat16)
```

```python
import functools

import jax
import jax.numpy as jnp
from jax import lax
from jax.experimental import pallas as pl
from jax.experimental.pallas import tpu as pltpu
from jax.sharding import PartitionSpec as P

DK = 128
DV = 128
CK = 3
BLK = 64
LANES = 128
PAD = 8


EPS = 1e-06
F32 = jnp.float32
BF16 = jnp.bfloat16
MESH = pl.DeviceIdType.MESH


def rms_scale(value_rows):
    return lax.rsqrt(jnp.mean(value_rows * value_rows, axis=-1, keepdims=True) + EPS)


def nt_dot(a, b):
    return lax.dot_general(a, b, (((1,), (1,)), ((), ())), preferred_element_type=F32)


def tn_dot(a, b):
    return lax.dot_general(a, b, (((0,), (0,)), ((), ())), preferred_element_type=F32)


def tp_places():
    me = lax.axis_index("tp")
    pair, core = me // 2, me % 2
    partner = 2 * pair + (1 - core)
    cross = 2 * (1 - pair) + core
    far = 2 * (1 - pair) + (1 - core)
    return me, partner, cross, far


def aligned(start, size):
    return pl.ds(pl.multiple_of(start, size), size)


def aligned_by(start, step, size):
    return pl.ds(pl.multiple_of(start, step), size)


def row_of(ref):
    lines = ref[...].astype(F32)
    return jnp.concatenate([lines[i : i + 1, :] for i in range(lines.shape[0])], axis=1)


def layer_kernel(
    heads,
    chunk,
    pieces,
    x_hbm,
    gain_hbm,
    wq_hbm,
    wf_hbm,
    wv_hbm,
    wpre_hbm,
    wconv_hbm,
    wpost_hbm,
    wout_hbm,
    surge_hbm,
    fmin_hbm,
    taps_hbm,
    hgain_hbm,
    start_hbm,
    wr_hbm,
    wc_hbm,
    ogain_hbm,
    out_ref,
    wbuf,
    xg,
    nb,
    surge,
    part,
    shift,
    st,
    run,
    pack,
    decs,
    land,
    land_decay,
    ent,
    back,
    gate,
    post,
    mix,
    halo,
    wr,
    wc,
    acc,
    pbuf,
    prcv,
    cbuf,
    crcv,
    land_state,
    gain_ref,
    fmin_ref,
    taps_ref,
    hgain_ref,
    start_ref,
    ogain_ref,
    lsem,
    csend,
    crecv,
    psend,
    precv,
    fsend,
    frecv,
    s1,
    r1,
    sd,
    rd,
    s2,
    r2,
    hs,
    hr,
    ps,
    pr,
    cs,
    cr,
    ready,
):
    peers, tokens, width = xg.shape
    steps = tokens // chunk
    sp = lax.axis_size("sp")
    seq = lax.axis_index("sp")
    quarter = tokens // peers
    size = quarter // pieces
    me, partner, cross, far = tp_places()
    sources = (wq_hbm, wf_hbm, wv_hbm, wpre_hbm, wconv_hbm, wpost_hbm, wout_hbm)

    x_copy = pltpu.make_async_copy(x_hbm, xg.at[me], lsem.at[0])
    surge_copy = pltpu.make_async_copy(surge_hbm, surge, lsem.at[1])
    wr_copy = pltpu.make_async_copy(wr_hbm, wr, lsem.at[2])
    wc_copy = pltpu.make_async_copy(wc_hbm, wc, lsem.at[3])

    def weight_copy(j):
        return pltpu.make_async_copy(sources[j], wbuf.at[j], lsem.at[4 + j])

    x_copy.start()
    smalls = (
        (gain_hbm, gain_ref),
        (fmin_hbm, fmin_ref),
        (taps_hbm, taps_ref),
        (hgain_hbm, hgain_ref),
        (start_hbm, start_ref),
        (ogain_hbm, ogain_ref),
    )
    small_copies = [
        pltpu.make_async_copy(src, dst, lsem.at[11 + i]) for i, (src, dst) in enumerate(smalls)
    ]
    barrier = pltpu.get_barrier_semaphore()
    for other in (partner, cross):
        pl.semaphore_signal(barrier, inc=1, device_id={"tp": other}, device_id_type=MESH)
    for off in range(1, sp):
        to = (seq + off) % sp

        @pl.when(to > seq)
        def _():
            pl.semaphore_signal(barrier, inc=1, device_id={"sp": to}, device_id_type=MESH)

    for copy in small_copies:
        copy.start()
    for j in range(3):
        weight_copy(j).start()
    surge_copy.start()
    with jax.named_scope("entry"):
        x_copy.wait()
        pl.semaphore_wait(barrier, 2 + seq)

    def give(src, dst, send, recv, to):
        return pltpu.make_async_remote_copy(
            src_ref=src,
            dst_ref=dst,
            send_sem=send,
            recv_sem=recv,
            device_id=to,
            device_id_type=MESH,
        )

    def hop(step, slot, to, send, recv):
        rows = aligned(step * chunk, chunk)
        return give(xg.at[slot, rows], xg.at[slot, rows], send.at[step], recv.at[step], {"tp": to})

    for step in range(steps):
        hop(step, me, cross, csend, crecv).start()
    for step in range(steps):
        hop(step, me, partner, psend, precv).start()
    for j in range(3, 7):
        weight_copy(j).start()
    wc_copy.start()
    wr_copy.start()

    def state_hop(src, dst, slot, to, send, recv):
        return give(src.at[to], dst.at[slot], send.at[to], recv.at[slot], {"sp": to})

    def decay_hop(slot, to):
        return give(decs, land_decay.at[slot], sd.at[to], rd.at[slot], {"sp": to})

    for off in range(1, sp):
        to = (seq + off) % sp

        @pl.when(to < seq)
        def _():
            pl.semaphore_signal(ready, inc=1, device_id={"sp": to}, device_id_type=MESH)

    for copy in small_copies:
        copy.wait()
    running = [start_ref[h] for h in range(heads)]
    for h in range(heads):
        ent[0, h] = running[h].astype(BF16)

    @pl.when(seq > 0)
    def _():
        state_hop(ent, back, seq, 0, s2, r2).start()

    st[...] = jnp.zeros_like(st)
    run[...] = jnp.zeros_like(run)
    gain = row_of(gain_ref)
    row = lax.broadcasted_iota(jnp.int32, (BLK, BLK), 0)
    col = lax.broadcasted_iota(jnp.int32, (BLK, BLK), 1)
    causal = col <= row
    middle = (causal.astype(F32) - (col < BLK // 2).astype(F32)).astype(BF16)
    middle = jnp.concatenate([middle] * 3, axis=1)

    def block(rows, query_raw, forget_raw, values):
        forget = forget_raw.astype(F32)
        keys = (1.0 - fmin_ref[...]) * jax.nn.sigmoid(-forget)
        logs = jnp.log1p(-keys) + surge[rows, :]
        high = logs.astype(BF16)
        rest = logs - high.astype(F32)
        next_term = rest.astype(BF16)
        low = (rest - next_term.astype(F32)).astype(BF16)
        terms = jnp.concatenate([high, next_term, low], axis=0)
        rel = jnp.dot(middle, terms, preferred_element_type=F32)
        mid = logs[0:1, :] - rel[0:1, :]
        tail = rel[BLK - 1 : BLK, :]
        raw = query_raw.astype(F32)
        queries = raw * jax.nn.sigmoid(raw) * DK ** (-0.5)
        q_mid = queries * jnp.exp(rel)
        k_mid = keys * jnp.exp(-rel)
        q_in = q_mid * jnp.exp(mid)
        k_out = (k_mid * jnp.exp(tail)).astype(BF16)
        whole = jnp.exp(mid + tail)
        shift[rows, :] = (q_in * jnp.exp(run[...])).astype(BF16)
        run[...] = run[...] + mid + tail
        q_mid = q_mid.astype(BF16)
        k_mid = k_mid.astype(BF16)
        q_in = q_in.astype(BF16)
        for h in range(heads):
            ch = slice(h * DK, (h + 1) * DK)
            scores = jnp.where(causal, nt_dot(q_mid[:, ch], k_mid[:, ch]), 0.0).astype(BF16)
            before = st[h]
            part[rows, ch] = jnp.dot(
                scores, values[:, ch], preferred_element_type=F32
            ) + nt_dot(q_in[:, ch], before.astype(BF16))
            st[h] = before * whole[:, ch] + tn_dot(values[:, ch], k_out[:, ch])

    def project(rows, j):
        return jnp.dot(nb[rows, :], wbuf[j], preferred_element_type=F32).astype(BF16)

    lag = me % 2

    @pl.loop(0, steps + lag)
    def _(step):
        @pl.when(step < steps)
        def _():
            with jax.named_scope("wait_cross"):
                hop(step, cross, cross, csend, crecv).wait_recv()
            hop(step, cross, partner, fsend, frecv).start()

        @pl.when(step >= lag)
        def _():
            now = step - lag
            with jax.named_scope("wait_forward"):
                hop(now, partner, partner, psend, precv).wait_recv()
                hop(now, far, partner, fsend, frecv).wait_recv()
            rows = aligned(now * chunk, chunk)
            total = jnp.zeros((chunk, 1), F32)
            for s in range(peers):
                piece = xg[s, rows].astype(F32)
                total = total + jnp.sum(piece * piece, axis=-1, keepdims=True)
            scale = lax.rsqrt(total / (peers * width) + EPS)
            for s in range(peers):
                cols = slice(s * width, (s + 1) * width)
                nb[rows, cols] = (xg[s, rows].astype(F32) * scale * gain[:, cols]).astype(BF16)

            @pl.when(now == 0)
            def _():
                surge_copy.wait()
                for j in range(3):
                    weight_copy(j).wait()

            query_raw, forget_raw, value_raw = (project(rows, j) for j in range(3))
            for b in range(chunk // BLK):
                inner = slice(b * BLK, (b + 1) * BLK)
                block(
                    aligned(now * chunk + b * BLK, BLK),
                    query_raw[inner],
                    forget_raw[inner],
                    value_raw[inner],
                )

    piece = DK // sp
    packing = jax.named_scope("pack")
    packing.__enter__()
    whole = jnp.exp(run[...])
    for h in range(heads):
        ch = slice(h * DK, (h + 1) * DK)
        decs[h : h + 1, :] = whole[:, ch]
        state = st[h].T
        for p in range(sp):
            pack[p, h] = state[p * piece : (p + 1) * piece].astype(BF16)

    @pl.when(seq < sp - 1)
    def _():
        pl.semaphore_wait(ready, sp - 1 - seq)
        for off in range(1, sp):
            to = (seq + off) % sp
            decay_hop(seq, to).start()
            state_hop(pack, land, seq, to, s1, r1).start()

    land[seq] = pack[seq]
    land_decay[seq] = decs[...]
    packing.__exit__(None, None, None)
    gates = jax.named_scope("gates_a")
    gates.__enter__()
    for j in range(3, 7):
        weight_copy(j).wait()

    def halo_hop():
        return give(
            mix.at[pl.ds(tokens, PAD)], halo, hs.at[0], hr.at[0], {"sp": (seq + 1) % sp}
        )

    wide = 2 * chunk if tokens % (2 * chunk) == 0 else chunk

    @pl.loop(0, tokens // wide)
    def _(i):
        rows = aligned(i * wide, wide)
        mix[pl.ds(pl.multiple_of(PAD + i * wide, PAD), wide), :] = project(rows, 3).astype(
            F32
        ) * project(rows, 4).astype(F32)

    @pl.when(seq < sp - 1)
    def _():
        halo_hop().start()

    def prepare(which):
        rows = aligned(which * quarter, quarter)
        post[rows, :] = project(rows, 5)
        gate[rows, :] = project(rows, 6)

    def convolve(which):
        rows = aligned(which * quarter, quarter)
        near = mix[aligned_by(which * quarter, PAD, quarter + PAD), :]
        total = None
        for j in range(CK):
            first = PAD + j - (CK - 1)
            term = near[first : first + quarter, :] * taps_ref[j : j + 1, :].astype(F32)
            total = term if total is None else total + term
        conv = (post[rows, :].astype(F32) * total).astype(BF16)
        acc[rows, :] = jnp.dot(conv, wc[...], preferred_element_type=F32)

    prepare(far)
    gates.__exit__(None, None, None)
    with jax.named_scope("wait_states"):
        for off in range(1, sp):
            src = (seq + sp - off) % sp

            @pl.when(src < sp - 1)
            def _():
                decay_hop(src, (seq + off) % sp).wait_recv()
                state_hop(pack, land, src, (seq + off) % sp, s1, r1).wait_recv()

    gates = jax.named_scope("gates_b")
    gates.__enter__()
    lane = lax.broadcasted_iota(jnp.int32, (piece, DK), 1)
    pick = lane == seq * piece + lax.broadcasted_iota(jnp.int32, (piece, DK), 0)
    for i in range(sp - 1):
        for h in range(heads):
            line = jnp.broadcast_to(land_decay[i, h : h + 1, :], (piece, DK))
            decay = jnp.sum(jnp.where(pick, line, 0.0), axis=-1, keepdims=True)
            running[h] = decay * running[h] + land[i, h].astype(F32)
            ent[i + 1, h] = running[h].astype(BF16)
    back[seq] = ent[seq]
    for off in range(1, sp):
        to = (seq + off) % sp

        @pl.when(to > 0)
        def _():
            state_hop(ent, back, seq, to, s2, r2).start()

    prepare(cross)
    mix[0:PAD, :] = jnp.zeros((PAD, width), F32)

    @pl.when(seq > 0)
    def _():
        halo_hop().wait_recv()
        mix[0:PAD, :] = halo[...]

    wc_copy.wait()
    wr_copy.wait()
    convolve(far)
    convolve(cross)
    gates.__exit__(None, None, None)
    with jax.named_scope("wait_entering"):
        for off in range(1, sp):
            src = (seq + sp - off) % sp
            state_hop(ent, back, src, (seq + off) % sp, s2, r2).wait_recv()
    for h in range(heads):
        land_state[h] = jnp.concatenate(
            [back[i, h].astype(F32) for i in range(sp)], axis=0
        ).astype(BF16)

    def mixed(which, s):
        rows = aligned(which * quarter + s * size, size)
        gated = []
        for h in range(heads):
            ch = slice(h * DV, (h + 1) * DV)
            recur = part[rows, ch] + jnp.dot(
                shift[rows, ch], land_state[h], preferred_element_type=F32
            )
            g = gate[rows, ch].astype(F32)
            gated.append(
                (
                    recur * rms_scale(recur) * hgain_ref[...].astype(F32) * (g * jax.nn.sigmoid(g))
                ).astype(BF16)
            )
        rec = jnp.concatenate(gated, axis=1)
        return acc[rows, :] + jnp.dot(rec, wr[...], preferred_element_type=F32)

    def put(which, s):
        rows = aligned(which * quarter + s * size, size)
        acc[rows, :] = mixed(which, s)

    def partner_hop(i):
        return give(pbuf.at[i], prcv.at[i], ps.at[i], pr.at[i], {"tp": partner})

    def cross_hop(i):
        return give(cbuf.at[i], crcv.at[i], cs.at[i], cr.at[i], {"tp": cross})

    def share(which, s, slot):
        pbuf[slot] = mixed(which, s).astype(BF16)
        partner_hop(slot).start()

    def forward(s):
        partner_hop(s).wait_recv()
        rows = aligned(cross * quarter + s * size, size)
        cbuf[s] = (acc[rows, :] + prcv[s].astype(F32)).astype(BF16)
        cross_hop(s).start()

    sums = jax.named_scope("sums")
    sums.__enter__()

    @pl.loop(0, pieces + 1)
    def _(s):
        @pl.when(s < pieces)
        def _():
            share(far, s, s)

        @pl.when(s > 0)
        def _():
            forward(s - 1)

        @pl.when(s < pieces)
        def _():
            put(cross, s)

    prepare(partner)
    convolve(partner)
    prepare(me)
    convolve(me)

    @pl.loop(0, pieces)
    def _(s):
        share(partner, s, pieces + s)
        put(me, s)

    sums.__exit__(None, None, None)
    last = jax.named_scope("last")
    last.__enter__()
    ogain = row_of(ogain_ref)

    @pl.loop(0, pieces)
    def _(s):
        partner_hop(pieces + s).wait_recv()
        cross_hop(s).wait_recv()
        rows = aligned(me * quarter + s * size, size)
        total = acc[rows, :] + prcv[pieces + s].astype(F32) + crcv[s].astype(F32)
        out_ref[aligned(s * size, size), :] = (total * rms_scale(total) * ogain).astype(BF16)

    last.__exit__(None, None, None)
    for step in range(steps):
        hop(step, me, cross, csend, crecv).wait_send()
        hop(step, me, partner, psend, precv).wait_send()
        hop(step, cross, partner, fsend, frecv).wait_send()
    for off in range(1, sp):
        to = (seq + off) % sp

        @pl.when(seq < sp - 1)
        def _():
            decay_hop(seq, to).wait_send()
            state_hop(pack, land, seq, to, s1, r1).wait_send()

        state_hop(ent, back, seq, to, s2, r2).wait_send()

    @pl.when(seq < sp - 1)
    def _():
        halo_hop().wait_send()

    for i in range(2 * pieces):
        partner_hop(i).wait_send()
    for i in range(pieces):
        cross_hop(i).wait_send()


def shards(
    layer_input,
    input_norm_gain,
    query_weight,
    forget_weight,
    value_matrix,
    output_gate_weight,
    after_gate_weight,
    before_gate_weight,
    convolution_input_weight,
    forget_minimum,
    surge_log_decay,
    convolution_kernel,
    head_norm_gain,
    starting_state,
    recurrence_output_weight,
    convolution_output_weight,
    output_norm_gain,
):
    sp, tp = lax.axis_size("sp"), lax.axis_size("tp")
    tokens, width = layer_input.shape
    wide = recurrence_output_weight.shape[1]
    depth, cols = query_weight.shape
    heads = cols // DV
    chunk = 128 if tokens % 128 == 0 else BLK
    steps = tokens // chunk
    quarter = tokens // tp
    pieces = 4 if quarter % 64 == 0 else 2
    size = quarter // pieces
    shares = (sp, heads, DK // sp, DV)
    vmem = pl.BlockSpec(memory_space=pltpu.VMEM)
    hbm = pl.BlockSpec(memory_space=pltpu.HBM)
    dma = pltpu.SemaphoreType.DMA
    return pl.pallas_call(
        functools.partial(layer_kernel, heads, chunk, pieces),
        out_shape=pltpu.VMEM((quarter, wide), BF16),
        in_specs=[hbm] * 17,
        out_specs=vmem,
        scratch_shapes=[
            pltpu.VMEM((7, depth, cols), BF16),
            pltpu.VMEM((tp, tokens, width), BF16),
            pltpu.VMEM((tokens, depth), BF16),
            pltpu.VMEM((tokens, cols), F32),
            pltpu.VMEM((tokens, cols), F32),
            pltpu.VMEM((tokens, cols), BF16),
            pltpu.VMEM((heads, DV, DK), F32),
            pltpu.VMEM((1, cols), F32),
            pltpu.VMEM(shares, BF16),
            pltpu.VMEM((heads, DK), F32),
            pltpu.VMEM(shares, BF16),
            pltpu.VMEM((sp, heads, DK), F32),
            pltpu.VMEM(shares, BF16),
            pltpu.VMEM(shares, BF16),
            pltpu.VMEM((tokens, cols), BF16),
            pltpu.VMEM((tokens, cols), BF16),
            pltpu.VMEM((tokens + PAD, cols), F32),
            pltpu.VMEM((PAD, cols), F32),
            pltpu.VMEM((cols, wide), BF16),
            pltpu.VMEM((cols, wide), BF16),
            pltpu.VMEM((tokens, wide), F32),
            pltpu.VMEM((2 * pieces, size, wide), BF16),
            pltpu.VMEM((2 * pieces, size, wide), BF16),
            pltpu.VMEM((pieces, size, wide), BF16),
            pltpu.VMEM((pieces, size, wide), BF16),
            pltpu.VMEM((heads, DK, DV), BF16),
            pltpu.VMEM((depth // LANES, LANES), BF16),
            pltpu.VMEM((1, cols), F32),
            pltpu.VMEM((CK, cols), BF16),
            pltpu.VMEM((1, DV), BF16),
            pltpu.VMEM(starting_state.shape, F32),
            pltpu.VMEM((wide // LANES, LANES), BF16),
            dma((17,)),
        ]
        + [dma((steps,))] * 6
        + [dma((sp,))] * 6
        + [dma((1,))] * 2
        + [dma((2 * pieces,))] * 2
        + [dma((pieces,))] * 2
        + [pltpu.SemaphoreType.REGULAR],
        compiler_params=pltpu.CompilerParams(collective_id=0, has_side_effects=True, vmem_limit_bytes=56 * 1024 * 1024),
        name="layer",
    )(
        layer_input,
        input_norm_gain.reshape(-1, LANES),
        query_weight,
        forget_weight,
        value_matrix,
        before_gate_weight,
        convolution_input_weight,
        after_gate_weight,
        output_gate_weight,
        surge_log_decay,
        forget_minimum[None, :],
        convolution_kernel,
        head_norm_gain[None, :],
        starting_state,
        recurrence_output_weight,
        convolution_output_weight,
        output_norm_gain.reshape(-1, LANES),
    )


def solution(mesh):
    return jax.shard_map(
        shards,
        mesh=mesh,
        in_specs=(
            P("sp", "tp"),
            P(),
            P(None, "tp"),
            P(None, "tp"),
            P(None, "tp"),
            P(None, "tp"),
            P(None, "tp"),
            P(None, "tp"),
            P(None, "tp"),
            P("tp"),
            P("sp", "tp"),
            P(None, "tp"),
            P(),
            P("tp", "sp", None),
            P("tp", None),
            P("tp", None),
            P(),
        ),
        out_specs=P(("sp", "tp"), None),
        check_vma=False,
    )
```

```python
import functools

import jax
import jax.numpy as jnp
from jax import lax
from jax.experimental import pallas as pl
from jax.experimental.pallas import tpu as pltpu
from jax.sharding import PartitionSpec as P

DK = 128
DV = 128
CK = 3
BLK = 64
LANES = 128
PAD = 8


EPS = 1e-06
F32 = jnp.float32
BF16 = jnp.bfloat16
MESH = pl.DeviceIdType.MESH


def rms_scale(value_rows):
    return lax.rsqrt(jnp.mean(value_rows * value_rows, axis=-1, keepdims=True) + EPS)


def nt_dot(a, b):
    return lax.dot_general(a, b, (((1,), (1,)), ((), ())), preferred_element_type=F32)


def tn_dot(a, b):
    return lax.dot_general(a, b, (((0,), (0,)), ((), ())), preferred_element_type=F32)


def split_terms(logs):
    high = logs.astype(BF16)
    rest = logs - high.astype(F32)
    next_term = rest.astype(BF16)
    low = (rest - next_term.astype(F32)).astype(BF16)
    return jnp.concatenate([high, next_term, low], axis=0)


def tp_places():
    me = lax.axis_index("tp")
    pair, core = me // 2, me % 2
    partner = 2 * pair + (1 - core)
    cross = 2 * (1 - pair) + core
    far = 2 * (1 - pair) + (1 - core)
    return me, partner, cross, far


def owner_place(sp):
    owners = max(1, sp // 2)
    return (sp - owners) // 2, sp // owners


def outward(low, high):
    order = []
    while low <= high:
        order += [low, high] if low < high else [low]
        low, high = low + 1, high - 1
    return order


def aligned(start, size):
    return pl.ds(pl.multiple_of(start, size), size)


def aligned_by(start, step, size):
    return pl.ds(pl.multiple_of(start, step), size)


def row_of(ref):
    lines = ref[...].astype(F32)
    return jnp.concatenate([lines[i : i + 1, :] for i in range(lines.shape[0])], axis=1)


def layer_kernel(
    heads,
    chunk,
    pieces,
    x_hbm,
    gain_hbm,
    wq_hbm,
    wf_hbm,
    wv_hbm,
    wpre_hbm,
    wconv_hbm,
    wpost_hbm,
    wout_hbm,
    surge_hbm,
    fmin_hbm,
    taps_hbm,
    hgain_hbm,
    start_hbm,
    wr_hbm,
    wc_hbm,
    ogain_hbm,
    out_ref,
    wbuf,
    xg,
    nb,
    surge,
    part,
    shift,
    st,
    run,
    raw,
    carry,
    pair_land,
    pair_decs,
    pair_factor,
    start_land,
    pack,
    decs,
    land,
    land_decay,
    ent,
    back,
    gate,
    post,
    mix,
    halo,
    wr,
    wc,
    acc,
    pbuf,
    prcv,
    cbuf,
    crcv,
    land_state,
    gain_ref,
    fmin_ref,
    taps_ref,
    hgain_ref,
    start_ref,
    ogain_ref,
    lsem,
    csend,
    crecv,
    psend,
    precv,
    fsend,
    frecv,
    s1,
    r1,
    sd,
    rd,
    s2,
    r2,
    hs,
    hr,
    ps,
    pr,
    cs,
    cr,
    ready,
    ss,
    sr,
    qs,
    qr,
):
    peers, tokens, width = xg.shape
    groups, team = decs.shape[:2]
    owners, piece = back.shape[0], back.shape[3]
    first_owner, ratio = owner_place(lax.axis_size("sp"))
    steps = tokens // chunk
    sp = lax.axis_size("sp")
    seq = lax.axis_index("sp")
    quarter = tokens // peers
    size = quarter // pieces
    me, partner, cross, far = tp_places()
    sources = (wq_hbm, wf_hbm, wv_hbm, wpre_hbm, wconv_hbm, wpost_hbm, wout_hbm)

    x_copy = pltpu.make_async_copy(x_hbm, xg.at[me], lsem.at[0])
    surge_copy = pltpu.make_async_copy(surge_hbm, surge, lsem.at[1])
    wr_copy = pltpu.make_async_copy(wr_hbm, wr, lsem.at[2])
    wc_copy = pltpu.make_async_copy(wc_hbm, wc, lsem.at[3])

    def weight_copy(j):
        return pltpu.make_async_copy(sources[j], wbuf.at[j], lsem.at[4 + j])

    x_copy.start()
    smalls = (
        (gain_hbm, gain_ref),
        (fmin_hbm, fmin_ref),
        (taps_hbm, taps_ref),
        (hgain_hbm, hgain_ref),
        (start_hbm, start_ref),
        (ogain_hbm, ogain_ref),
    )
    small_copies = [
        pltpu.make_async_copy(src, dst, lsem.at[11 + i]) for i, (src, dst) in enumerate(smalls)
    ]
    barrier = pltpu.get_barrier_semaphore()
    for other in (partner, cross):
        pl.semaphore_signal(barrier, inc=1, device_id={"tp": other}, device_id_type=MESH)
    for off in range(1, sp):
        to = (seq + off) % sp

        @pl.when(to > seq)
        def _():
            pl.semaphore_signal(barrier, inc=1, device_id={"sp": to}, device_id_type=MESH)

    for copy in small_copies:
        copy.start()
    for j in range(3):
        weight_copy(j).start()
    surge_copy.start()
    with jax.named_scope("entry"):
        x_copy.wait()
        pl.semaphore_wait(barrier, 2 + seq)

    def give(src, dst, send, recv, to):
        return pltpu.make_async_remote_copy(
            src_ref=src,
            dst_ref=dst,
            send_sem=send,
            recv_sem=recv,
            device_id=to,
            device_id_type=MESH,
        )

    def hop(step, slot, to, send, recv):
        rows = aligned(step * chunk, chunk)
        return give(xg.at[slot, rows], xg.at[slot, rows], send.at[step], recv.at[step], {"tp": to})

    for step in range(steps):
        hop(step, me, cross, csend, crecv).start()
    for step in range(steps):
        hop(step, me, partner, psend, precv).start()
    for j in range(3, 7):
        weight_copy(j).start()
    wc_copy.start()
    wr_copy.start()

    own = jnp.clip(seq - first_owner, 0, owners - 1)
    is_owner = (seq >= first_owner) & (seq < first_owner + owners)
    start_owner = first_owner + seq // ratio

    def state_hop(g, k, slot, to):
        return give(pack.at[k, g], land.at[slot, g], s1.at[g, k], r1.at[g, slot], {"sp": to})

    def decay_hop(g, k, slot, to):
        return give(decs.at[g], land_decay.at[slot, g], sd.at[g, k], rd.at[g, slot], {"sp": to})

    def enter_hop(g, i, slot, to):
        return give(ent.at[i, g], back.at[slot, g], s2.at[g, to], r2.at[g, slot], {"sp": to})

    def pair_hop():
        return give(pack, pair_land, qs.at[0], qr.at[0], {"sp": (seq + 1) % sp})

    def pair_decay_hop():
        return give(decs, pair_decs, qs.at[1], qr.at[1], {"sp": (seq + 1) % sp})

    def start_hop(slot):
        return give(
            start_ref, start_land.at[slot], ss.at[0], sr.at[slot], {"sp": start_owner}
        )

    for off in range(1, sp):
        to = (seq + off) % sp

        @pl.when(to < seq)
        def _():
            pl.semaphore_signal(ready, inc=1, device_id={"sp": to}, device_id_type=MESH)

    for copy in small_copies:
        copy.wait()

    st[...] = jnp.zeros_like(st)
    run[...] = jnp.zeros_like(run)
    gain = row_of(gain_ref)
    row = lax.broadcasted_iota(jnp.int32, (BLK, BLK), 0)
    col = lax.broadcasted_iota(jnp.int32, (BLK, BLK), 1)
    causal = col <= row
    middle = (causal.astype(F32) - (col < BLK // 2).astype(F32)).astype(BF16)
    middle = jnp.concatenate([middle] * 3, axis=1)

    def block(rows, query_raw, forget_raw, values):
        forget = forget_raw.astype(F32)
        keys = (1.0 - fmin_ref[...]) * jax.nn.sigmoid(-forget)
        logs = jnp.log1p(-keys) + surge[rows, :]
        rel = jnp.dot(middle, split_terms(logs), preferred_element_type=F32)
        mid = logs[0:1, :] - rel[0:1, :]
        tail = rel[BLK - 1 : BLK, :]
        raw = query_raw.astype(F32)
        queries = raw * jax.nn.sigmoid(raw) * DK ** (-0.5)
        q_mid = queries * jnp.exp(rel)
        k_mid = keys * jnp.exp(-rel)
        q_in = q_mid * jnp.exp(mid)
        k_out = (k_mid * jnp.exp(tail)).astype(BF16)
        whole = jnp.exp(mid + tail)
        shift[rows, :] = (q_in * jnp.exp(run[...])).astype(BF16)
        run[...] = run[...] + mid + tail
        q_mid = q_mid.astype(BF16)
        k_mid = k_mid.astype(BF16)
        q_in = q_in.astype(BF16)
        for h in range(heads):
            ch = slice(h * DK, (h + 1) * DK)
            scores = jnp.where(causal, nt_dot(q_mid[:, ch], k_mid[:, ch]), 0.0).astype(BF16)
            before = st[h]
            part[rows, ch] = jnp.dot(
                scores, values[:, ch], preferred_element_type=F32
            ) + nt_dot(q_in[:, ch], before.astype(BF16))
            st[h] = before * whole[:, ch] + tn_dot(values[:, ch], k_out[:, ch])

    def project(rows, j):
        return jnp.dot(nb[rows, :], wbuf[j], preferred_element_type=F32).astype(BF16)

    def blend(rows, now):
        mix[aligned_by(PAD + now * chunk, PAD, chunk), :] = project(rows, 3).astype(
            F32
        ) * project(rows, 4).astype(F32)

    def arrive(now):
        with jax.named_scope("wait_forward"):
            hop(now, partner, partner, psend, precv).wait_recv()
            hop(now, far, partner, fsend, frecv).wait_recv()
        rows = aligned(now * chunk, chunk)
        total = jnp.zeros((chunk, 1), F32)
        for s in range(peers):
            part_x = xg[s, rows].astype(F32)
            total = total + jnp.sum(part_x * part_x, axis=-1, keepdims=True)
        scale = lax.rsqrt(total / (peers * width) + EPS)
        for s in range(peers):
            cols = slice(s * width, (s + 1) * width)
            nb[rows, cols] = (xg[s, rows].astype(F32) * scale * gain[:, cols]).astype(BF16)
        return rows

    def blocks(now, query_raw, forget_raw, value_raw):
        for b in range(chunk // BLK):
            inner = slice(b * BLK, (b + 1) * BLK)
            block(
                aligned(now * chunk + b * BLK, BLK),
                query_raw[inner],
                forget_raw[inner],
                value_raw[inner],
            )

    lag = me % 2

    @pl.loop(0, steps + lag)
    def _(step):
        @pl.when(step < steps)
        def _():
            with jax.named_scope("wait_cross"):
                hop(step, cross, cross, csend, crecv).wait_recv()
            hop(step, cross, partner, fsend, frecv).start()

        @pl.when((step >= lag) & (step < steps - 1 + lag))
        def _():
            now = step - lag
            rows = arrive(now)

            @pl.when(now == 0)
            def _():
                surge_copy.wait()
                for j in range(5):
                    weight_copy(j).wait()

            blocks(now, *(project(rows, j) for j in range(3)))
            blend(rows, now)

            @pl.when(now == 0)
            def _():
                @pl.when(seq < sp - 1)
                def _():
                    pl.semaphore_wait(ready, sp - 1 - seq)

                @pl.when(seq != start_owner)
                def _():
                    start_hop(seq % ratio).start()

                @pl.when(seq == start_owner)
                def _():
                    start_land[seq % ratio] = start_ref[...]

    def enter(i, g):
        for to in (i,) if i < sp - 2 else (i, i + 1):

            @pl.when(seq != to)
            def _():
                enter_hop(g, i, own, to).start()

            @pl.when(seq == to)
            def _():
                back[own, g] = ent[i, g]

    @pl.when(is_owner)
    def _():
        for r in range(ratio):

            @pl.when(seq != own * ratio + r)
            def _():
                start_hop(r).wait_recv()

        for g in range(groups):
            for t in range(team):
                running = jnp.concatenate(
                    [start_land[r, g * team + t] for r in range(ratio)], axis=0
                )
                carry[g, t] = running
                ent[0, g, t] = running.astype(BF16)
        for g in range(groups):
            enter(0, g)

    final = steps - 1
    rows = arrive(final)
    packing = jax.named_scope("pack")
    packing.__enter__()
    span = team * DK
    row = lax.broadcasted_iota(jnp.int32, (chunk, chunk), 0)
    col = lax.broadcasted_iota(jnp.int32, (chunk, chunk), 1)
    later = (col > row).astype(F32).astype(BF16)
    later = jnp.concatenate([later] * 3, axis=1)
    raw[0], raw[1] = project(rows, 1), project(rows, 2)
    for g in range(groups):
        cols = slice(g * span, (g + 1) * span)
        forget_raw, value_raw = raw[0, :, cols], raw[1, :, cols]
        keys = (1.0 - fmin_ref[:, cols]) * jax.nn.sigmoid(-forget_raw.astype(F32))
        logs = jnp.log1p(-keys) + surge[rows, cols]
        after = jnp.dot(later, split_terms(logs), preferred_element_type=F32)
        total = after[0:1, :] + logs[0:1, :]
        k_out = (keys * jnp.exp(after)).astype(BF16)
        whole = jnp.exp(total)
        gone = jnp.exp(run[:, cols] + total)
        for t in range(team):
            ch = slice(t * DK, (t + 1) * DK)
            decs[g, t : t + 1, :] = gone[:, ch]
            state = st[g * team + t] * whole[:, ch] + tn_dot(value_raw[:, ch], k_out[:, ch])
            state = state.T
            for k in range(owners):
                pack[k, g, t] = state[k * piece : (k + 1) * piece].astype(BF16)

        @pl.when(seq < sp - 2)
        def _():
            for k in range(owners):

                @pl.when(seq != first_owner + k)
                def _():
                    decay_hop(g, k, seq, first_owner + k).start()
                    state_hop(g, k, seq, first_owner + k).start()

    @pl.when(seq == sp - 2)
    def _():
        pair_decay_hop().start()
        pair_hop().start()

    @pl.when(is_owner & (seq < sp - 2))
    def _():
        land[seq] = pack[own]
        land_decay[seq] = decs[...]

    packing.__exit__(None, None, None)

    def combine(g, low, high):
        with jax.named_scope("wait_states"):
            for i in range(low, high):

                @pl.when(seq != i)
                def _():
                    decay_hop(g, 0, i, seq).wait_recv()
                    state_hop(g, 0, i, seq).wait_recv()

        lane = lax.broadcasted_iota(jnp.int32, (piece, DK), 1)
        pick = lane == own * piece + lax.broadcasted_iota(jnp.int32, (piece, DK), 0)
        for t in range(team):
            running = carry[g, t]
            for i in range(low, high):
                line = jnp.broadcast_to(land_decay[i, g, t : t + 1, :], (piece, DK))
                decay = jnp.sum(jnp.where(pick, line, 0.0), axis=-1, keepdims=True)
                running = decay * running + land[i, g, t].astype(F32)
                ent[i + 1, g, t] = running.astype(BF16)
            carry[g, t] = running
        for i in outward(low + 1, high):
            enter(i, g)

    gates = jax.named_scope("gates_a")
    gates.__enter__()
    for j in range(5, 7):
        weight_copy(j).wait()
    blocks(final, project(rows, 0), raw[0], raw[1])
    blend(rows, final)

    def prepare(which):
        rows = aligned(which * quarter, quarter)
        post[rows, :] = project(rows, 5)
        gate[rows, :] = project(rows, 6)

    def convolve(which):
        rows = aligned(which * quarter, quarter)
        near = mix[aligned_by(which * quarter, PAD, quarter + PAD), :]
        total = None
        for j in range(CK):
            first = PAD + j - (CK - 1)
            term = near[first : first + quarter, :] * taps_ref[j : j + 1, :].astype(F32)
            total = term if total is None else total + term
        conv = (post[rows, :].astype(F32) * total).astype(BF16)
        acc[rows, :] = jnp.dot(conv, wc[...], preferred_element_type=F32)

    def halo_hop():
        return give(
            mix.at[pl.ds(tokens, PAD)], halo, hs.at[0], hr.at[0], {"sp": (seq + 1) % sp}
        )

    @pl.when(seq < sp - 1)
    def _():
        halo_hop().start()

    prepare(far)
    gates.__exit__(None, None, None)

    @pl.when(is_owner)
    def _():
        split = sp // 4
        for low, high in ((0, split), (split, sp - 2)):
            for g in range(groups):
                combine(g, low, high)

    gates = jax.named_scope("gates_c")
    gates.__enter__()
    prepare(cross)
    mix[0:PAD, :] = jnp.zeros((PAD, width), F32)

    @pl.when(seq > 0)
    def _():
        halo_hop().wait_recv()
        mix[0:PAD, :] = halo[...]

    wc_copy.wait()
    wr_copy.wait()
    convolve(far)
    convolve(cross)
    gates.__exit__(None, None, None)
    def whole_state(pieces_ref, h):
        return jnp.concatenate(
            [pieces_ref[k, h // team, h % team].astype(F32) for k in range(owners)], axis=0
        )

    @pl.when(seq == sp - 1)
    def _():
        pair_decay_hop().wait_recv()
        pair_hop().wait_recv()
        for h in range(heads):
            line = pair_decs[h // team, h % team : h % team + 1, :]
            pair_factor[h] = jnp.broadcast_to(line, (DV, DK)).T

    with jax.named_scope("wait_entering"):
        for g in range(groups):
            for k in range(owners):

                @pl.when(seq != first_owner + k)
                def _():
                    enter_hop(g, 0, k, 0).wait_recv()

    @pl.when(seq < sp - 1)
    def _():
        for h in range(heads):
            land_state[h] = whole_state(back, h).astype(BF16)

    @pl.when(seq == sp - 1)
    def _():
        for h in range(heads):
            land_state[h] = (
                pair_factor[h] * whole_state(back, h) + whole_state(pair_land, h)
            ).astype(BF16)

    def mixed(which, s):
        rows = aligned(which * quarter + s * size, size)
        gated = []
        for h in range(heads):
            ch = slice(h * DV, (h + 1) * DV)
            recur = part[rows, ch] + jnp.dot(
                shift[rows, ch], land_state[h], preferred_element_type=F32
            )
            g = gate[rows, ch].astype(F32)
            gated.append(
                (
                    recur * rms_scale(recur) * hgain_ref[...].astype(F32) * (g * jax.nn.sigmoid(g))
                ).astype(BF16)
            )
        rec = jnp.concatenate(gated, axis=1)
        return acc[rows, :] + jnp.dot(rec, wr[...], preferred_element_type=F32)

    def put(which, s):
        rows = aligned(which * quarter + s * size, size)
        acc[rows, :] = mixed(which, s)

    def partner_hop(i):
        return give(pbuf.at[i], prcv.at[i], ps.at[i], pr.at[i], {"tp": partner})

    def cross_hop(i):
        return give(cbuf.at[i], crcv.at[i], cs.at[i], cr.at[i], {"tp": cross})

    def share(which, s, slot):
        pbuf[slot] = mixed(which, s).astype(BF16)
        partner_hop(slot).start()

    def forward(s):
        partner_hop(s).wait_recv()
        rows = aligned(cross * quarter + s * size, size)
        cbuf[s] = (acc[rows, :] + prcv[s].astype(F32)).astype(BF16)
        cross_hop(s).start()

    sums = jax.named_scope("sums")
    sums.__enter__()

    @pl.loop(0, pieces + 1)
    def _(s):
        @pl.when(s < pieces)
        def _():
            share(far, s, s)

        @pl.when(s > 0)
        def _():
            forward(s - 1)

        @pl.when(s < pieces)
        def _():
            put(cross, s)

    prepare(partner)
    convolve(partner)
    prepare(me)
    convolve(me)

    @pl.loop(0, pieces)
    def _(s):
        share(partner, s, pieces + s)
        put(me, s)

    sums.__exit__(None, None, None)
    last = jax.named_scope("last")
    last.__enter__()
    ogain = row_of(ogain_ref)

    @pl.loop(0, pieces)
    def _(s):
        partner_hop(pieces + s).wait_recv()
        cross_hop(s).wait_recv()
        rows = aligned(me * quarter + s * size, size)
        total = acc[rows, :] + prcv[pieces + s].astype(F32) + crcv[s].astype(F32)
        out_ref[aligned(s * size, size), :] = (total * rms_scale(total) * ogain).astype(BF16)

    last.__exit__(None, None, None)
    for step in range(steps):
        hop(step, me, cross, csend, crecv).wait_send()
        hop(step, me, partner, psend, precv).wait_send()
        hop(step, cross, partner, fsend, frecv).wait_send()
    @pl.when(seq < sp - 2)
    def _():
        for g in range(groups):
            for k in range(owners):

                @pl.when(seq != first_owner + k)
                def _():
                    decay_hop(g, k, seq, first_owner + k).wait_send()
                    state_hop(g, k, seq, first_owner + k).wait_send()

    @pl.when(seq == sp - 2)
    def _():
        pair_decay_hop().wait_send()
        pair_hop().wait_send()

    @pl.when(is_owner)
    def _():
        for g in range(groups):
            for i in range(sp):

                @pl.when(seq != i)
                def _():
                    enter_hop(g, 0, own, i).wait_send()

    @pl.when(seq != start_owner)
    def _():
        start_hop(seq % ratio).wait_send()

    @pl.when(seq < sp - 1)
    def _():
        halo_hop().wait_send()

    for i in range(2 * pieces):
        partner_hop(i).wait_send()
    for i in range(pieces):
        cross_hop(i).wait_send()


def shards(
    layer_input,
    input_norm_gain,
    query_weight,
    forget_weight,
    value_matrix,
    output_gate_weight,
    after_gate_weight,
    before_gate_weight,
    convolution_input_weight,
    forget_minimum,
    surge_log_decay,
    convolution_kernel,
    head_norm_gain,
    starting_state,
    recurrence_output_weight,
    convolution_output_weight,
    output_norm_gain,
):
    sp, tp = lax.axis_size("sp"), lax.axis_size("tp")
    tokens, width = layer_input.shape
    wide = recurrence_output_weight.shape[1]
    depth, cols = query_weight.shape
    heads = cols // DV
    chunk = 128 if tokens % 128 == 0 else BLK
    steps = tokens // chunk
    quarter = tokens // tp
    pieces = 4 if quarter % 64 == 0 else 2
    size = quarter // pieces
    _, ratio = owner_place(sp)
    owners = sp // ratio
    groups = 2 if heads % 2 == 0 else 1
    team = heads // groups
    share = (groups, team, DK // owners, DV)
    vmem = pl.BlockSpec(memory_space=pltpu.VMEM)
    hbm = pl.BlockSpec(memory_space=pltpu.HBM)
    dma = pltpu.SemaphoreType.DMA
    return pl.pallas_call(
        functools.partial(layer_kernel, heads, chunk, pieces),
        out_shape=pltpu.VMEM((quarter, wide), BF16),
        in_specs=[hbm] * 17,
        out_specs=vmem,
        scratch_shapes=[
            pltpu.VMEM((7, depth, cols), BF16),
            pltpu.VMEM((tp, tokens, width), BF16),
            pltpu.VMEM((tokens, depth), BF16),
            pltpu.VMEM((tokens, cols), F32),
            pltpu.VMEM((tokens, cols), F32),
            pltpu.VMEM((tokens, cols), BF16),
            pltpu.VMEM((heads, DV, DK), F32),
            pltpu.VMEM((1, cols), F32),
            pltpu.VMEM((2, chunk, cols), BF16),
            pltpu.VMEM(share, F32),
            pltpu.VMEM((owners,) + share, BF16),
            pltpu.VMEM((groups, team, DK), F32),
            pltpu.VMEM((heads, DK, DV), F32),
            pltpu.VMEM((ratio,) + starting_state.shape, F32),
            pltpu.VMEM((owners,) + share, BF16),
            pltpu.VMEM((groups, team, DK), F32),
            pltpu.VMEM((sp,) + share, BF16),
            pltpu.VMEM((sp, groups, team, DK), F32),
            pltpu.VMEM((sp - 1,) + share, BF16),
            pltpu.VMEM((owners,) + share, BF16),
            pltpu.VMEM((tokens, cols), BF16),
            pltpu.VMEM((tokens, cols), BF16),
            pltpu.VMEM((tokens + PAD, cols), F32),
            pltpu.VMEM((PAD, cols), F32),
            pltpu.VMEM((cols, wide), BF16),
            pltpu.VMEM((cols, wide), BF16),
            pltpu.VMEM((tokens, wide), F32),
            pltpu.VMEM((2 * pieces, size, wide), BF16),
            pltpu.VMEM((2 * pieces, size, wide), BF16),
            pltpu.VMEM((pieces, size, wide), BF16),
            pltpu.VMEM((pieces, size, wide), BF16),
            pltpu.VMEM((heads, DK, DV), BF16),
            pltpu.VMEM((depth // LANES, LANES), BF16),
            pltpu.VMEM((1, cols), F32),
            pltpu.VMEM((CK, cols), BF16),
            pltpu.VMEM((1, DV), BF16),
            pltpu.VMEM(starting_state.shape, F32),
            pltpu.VMEM((wide // LANES, LANES), BF16),
            dma((17,)),
        ]
        + [dma((steps,))] * 6
        + [dma((groups, owners)), dma((groups, sp))] * 2
        + [dma((groups, sp)), dma((groups, owners))]
        + [dma((1,))] * 2
        + [dma((2 * pieces,))] * 2
        + [dma((pieces,))] * 2
        + [pltpu.SemaphoreType.REGULAR]
        + [dma((1,)), dma((ratio,)), dma((2,)), dma((2,))],
        compiler_params=pltpu.CompilerParams(collective_id=0, has_side_effects=True, vmem_limit_bytes=56 * 1024 * 1024),
        name="layer",
    )(
        layer_input,
        input_norm_gain.reshape(-1, LANES),
        query_weight,
        forget_weight,
        value_matrix,
        before_gate_weight,
        convolution_input_weight,
        after_gate_weight,
        output_gate_weight,
        surge_log_decay,
        forget_minimum[None, :],
        convolution_kernel,
        head_norm_gain[None, :],
        starting_state,
        recurrence_output_weight,
        convolution_output_weight,
        output_norm_gain.reshape(-1, LANES),
    )


def solution(mesh):
    return jax.shard_map(
        shards,
        mesh=mesh,
        in_specs=(
            P("sp", "tp"),
            P(),
            P(None, "tp"),
            P(None, "tp"),
            P(None, "tp"),
            P(None, "tp"),
            P(None, "tp"),
            P(None, "tp"),
            P(None, "tp"),
            P("tp"),
            P("sp", "tp"),
            P(None, "tp"),
            P(),
            P("tp", "sp", None),
            P("tp", None),
            P("tp", None),
            P(),
        ),
        out_specs=P(("sp", "tp"), None),
        check_vma=False,
    )
```

```python
import functools

import jax
import jax.numpy as jnp
from jax import lax
from jax.experimental import pallas as pl
from jax.experimental.pallas import tpu as pltpu
from jax.sharding import PartitionSpec as P

DK = 128
DV = 128
CK = 3
BLK = 64
LANES = 128
PAD = 8


EPS = 1e-06
F32 = jnp.float32
BF16 = jnp.bfloat16
MESH = pl.DeviceIdType.MESH


def rms_scale(value_rows):
    return lax.rsqrt(jnp.mean(value_rows * value_rows, axis=-1, keepdims=True) + EPS)


def nt_dot(a, b):
    return lax.dot_general(a, b, (((1,), (1,)), ((), ())), preferred_element_type=F32)


def tn_dot(a, b):
    return lax.dot_general(a, b, (((0,), (0,)), ((), ())), preferred_element_type=F32)


def split_terms(logs):
    high = logs.astype(BF16)
    rest = logs - high.astype(F32)
    next_term = rest.astype(BF16)
    low = (rest - next_term.astype(F32)).astype(BF16)
    return jnp.concatenate([high, next_term, low], axis=0)


def tp_places():
    me = lax.axis_index("tp")
    pair, core = me // 2, me % 2
    partner = 2 * pair + (1 - core)
    cross = 2 * (1 - pair) + core
    far = 2 * (1 - pair) + (1 - core)
    return me, partner, cross, far


def owner_place(sp):
    owners = max(1, sp // 2)
    return (sp - owners) // 2, sp // owners


def outward(low, high):
    order = []
    while low <= high:
        order += [low, high] if low < high else [low]
        low, high = low + 1, high - 1
    return order


def aligned(start, size):
    return pl.ds(pl.multiple_of(start, size), size)


def aligned_by(start, step, size):
    return pl.ds(pl.multiple_of(start, step), size)


def row_of(ref):
    lines = ref[...].astype(F32)
    return jnp.concatenate([lines[i : i + 1, :] for i in range(lines.shape[0])], axis=1)


def layer_kernel(
    heads,
    chunk,
    pieces,
    x_hbm,
    gain_hbm,
    wq_hbm,
    wf_hbm,
    wv_hbm,
    wpre_hbm,
    wconv_hbm,
    wpost_hbm,
    wout_hbm,
    surge_hbm,
    fmin_hbm,
    taps_hbm,
    hgain_hbm,
    start_hbm,
    wr_hbm,
    wc_hbm,
    ogain_hbm,
    out_ref,
    wbuf,
    xg,
    nb,
    surge,
    part,
    shift,
    st,
    run,
    raw,
    carry,
    pair_land,
    pair_decs,
    pair_factor,
    start_land,
    pack,
    decs,
    land,
    land_decay,
    ent,
    back,
    gate,
    post,
    mix,
    halo,
    wr,
    wc,
    acc,
    pbuf,
    prcv,
    cbuf,
    crcv,
    land_state,
    gain_ref,
    fmin_ref,
    taps_ref,
    hgain_ref,
    start_ref,
    ogain_ref,
    lsem,
    csend,
    crecv,
    psend,
    precv,
    fsend,
    frecv,
    s1,
    r1,
    sd,
    rd,
    s2,
    r2,
    hs,
    hr,
    ps,
    pr,
    cs,
    cr,
    ready,
    ss,
    sr,
    qs,
    qr,
):
    peers, tokens, width = xg.shape
    groups, team = decs.shape[:2]
    owners, piece = back.shape[0], back.shape[3]
    first_owner, ratio = owner_place(lax.axis_size("sp"))
    steps = tokens // chunk
    sp = lax.axis_size("sp")
    seq = lax.axis_index("sp")
    quarter = tokens // peers
    size = quarter // pieces
    me, partner, cross, far = tp_places()
    sources = (wq_hbm, wf_hbm, wv_hbm, wpre_hbm, wconv_hbm, wpost_hbm, wout_hbm)

    x_copy = pltpu.make_async_copy(x_hbm, xg.at[me], lsem.at[0])
    surge_copy = pltpu.make_async_copy(surge_hbm, surge, lsem.at[1])
    wr_copy = pltpu.make_async_copy(wr_hbm, wr, lsem.at[2])
    wc_copy = pltpu.make_async_copy(wc_hbm, wc, lsem.at[3])

    def weight_copy(j):
        return pltpu.make_async_copy(sources[j], wbuf.at[j], lsem.at[4 + j])

    x_copy.start()
    smalls = (
        (gain_hbm, gain_ref),
        (fmin_hbm, fmin_ref),
        (taps_hbm, taps_ref),
        (hgain_hbm, hgain_ref),
        (start_hbm, start_ref),
        (ogain_hbm, ogain_ref),
    )
    small_copies = [
        pltpu.make_async_copy(src, dst, lsem.at[11 + i]) for i, (src, dst) in enumerate(smalls)
    ]
    barrier = pltpu.get_barrier_semaphore()
    for other in (partner, cross):
        pl.semaphore_signal(barrier, inc=1, device_id={"tp": other}, device_id_type=MESH)
    for off in range(1, sp):
        to = (seq + off) % sp

        @pl.when(to > seq)
        def _():
            pl.semaphore_signal(barrier, inc=1, device_id={"sp": to}, device_id_type=MESH)

    for copy in small_copies:
        copy.start()
    for j in range(3):
        weight_copy(j).start()
    surge_copy.start()
    with jax.named_scope("entry"):
        x_copy.wait()
        pl.semaphore_wait(barrier, 2 + seq)

    def give(src, dst, send, recv, to):
        return pltpu.make_async_remote_copy(
            src_ref=src,
            dst_ref=dst,
            send_sem=send,
            recv_sem=recv,
            device_id=to,
            device_id_type=MESH,
        )

    def hop(step, slot, to, send, recv):
        rows = aligned(step * chunk, chunk)
        return give(xg.at[slot, rows], xg.at[slot, rows], send.at[0], recv.at[step], {"tp": to})

    def sent(slot, to, send, recv):
        give(xg.at[slot], xg.at[slot], send.at[0], recv.at[0], {"tp": to}).wait_send()

    def partner_copy(slot):
        return give(xg.at[slot], xg.at[slot], psend.at[0], precv.at[0], {"tp": partner})

    for step in range(steps):
        hop(step, me, cross, csend, crecv).start()
    partner_copy(me).start()
    for j in range(3, 7):
        weight_copy(j).start()
    wc_copy.start()
    wr_copy.start()

    own = jnp.clip(seq - first_owner, 0, owners - 1)
    is_owner = (seq >= first_owner) & (seq < first_owner + owners)
    start_owner = first_owner + seq // ratio

    split = sp // 4

    def stage_of(slot):
        return jnp.where(slot < split, 0, 1)

    def state_hop(g, k, slot, to):
        return give(
            pack.at[k, g], land.at[slot, g], s1.at[0], r1.at[g, stage_of(slot)], {"sp": to}
        )

    def decay_hop(slot, to):
        return give(decs, land_decay.at[slot], sd.at[0], rd.at[stage_of(slot)], {"sp": to})

    def enter_hop(g, i, slot, to):
        return give(ent.at[i, g], back.at[slot, g], s2.at[0], r2.at[0], {"sp": to})

    def pair_hop():
        return give(pack, pair_land, qs.at[0], qr.at[0], {"sp": (seq + 1) % sp})

    def pair_decay_hop():
        return give(decs, pair_decs, qs.at[1], qr.at[1], {"sp": (seq + 1) % sp})

    def start_hop(slot):
        return give(
            start_ref, start_land.at[slot], ss.at[0], sr.at[slot], {"sp": start_owner}
        )

    for off in range(1, sp):
        to = (seq + off) % sp

        @pl.when(to < seq)
        def _():
            pl.semaphore_signal(ready, inc=1, device_id={"sp": to}, device_id_type=MESH)

    for copy in small_copies:
        copy.wait()

    st[...] = jnp.zeros_like(st)
    run[...] = jnp.zeros_like(run)
    gain = row_of(gain_ref)
    row = lax.broadcasted_iota(jnp.int32, (BLK, BLK), 0)
    col = lax.broadcasted_iota(jnp.int32, (BLK, BLK), 1)
    causal = col <= row
    middle = (causal.astype(F32) - (col < BLK // 2).astype(F32)).astype(BF16)
    middle = jnp.concatenate([middle] * 3, axis=1)

    def block(rows, query_raw, forget_raw, values):
        forget = forget_raw.astype(F32)
        keys = (1.0 - fmin_ref[...]) * jax.nn.sigmoid(-forget)
        logs = jnp.log1p(-keys) + surge[rows, :]
        rel = jnp.dot(middle, split_terms(logs), preferred_element_type=F32)
        mid = logs[0:1, :] - rel[0:1, :]
        tail = rel[BLK - 1 : BLK, :]
        raw = query_raw.astype(F32)
        queries = raw * jax.nn.sigmoid(raw) * DK ** (-0.5)
        q_mid = queries * jnp.exp(rel)
        k_mid = keys * jnp.exp(-rel)
        q_in = q_mid * jnp.exp(mid)
        k_out = (k_mid * jnp.exp(tail)).astype(BF16)
        whole = jnp.exp(mid + tail)
        shift[rows, :] = (q_in * jnp.exp(run[...])).astype(BF16)
        run[...] = run[...] + mid + tail
        q_mid = q_mid.astype(BF16)
        k_mid = k_mid.astype(BF16)
        q_in = q_in.astype(BF16)
        for h in range(heads):
            ch = slice(h * DK, (h + 1) * DK)
            scores = jnp.where(causal, nt_dot(q_mid[:, ch], k_mid[:, ch]), 0.0).astype(BF16)
            before = st[h]
            part[rows, ch] = jnp.dot(
                scores, values[:, ch], preferred_element_type=F32
            ) + nt_dot(q_in[:, ch], before.astype(BF16))
            st[h] = before * whole[:, ch] + tn_dot(values[:, ch], k_out[:, ch])

    def project(rows, j):
        return jnp.dot(nb[rows, :], wbuf[j], preferred_element_type=F32).astype(BF16)

    def blend(rows, now):
        mix[aligned_by(PAD + now * chunk, PAD, chunk), :] = project(rows, 3).astype(
            F32
        ) * project(rows, 4).astype(F32)

    def arrive(now):
        with jax.named_scope("wait_forward"):
            hop(now, far, partner, fsend, frecv).wait_recv()
        rows = aligned(now * chunk, chunk)
        squares = jnp.zeros((chunk, width), F32)
        for s in range(peers):
            part_x = xg[s, rows].astype(F32)
            squares = squares + part_x * part_x
        total = jnp.sum(squares, axis=-1, keepdims=True)
        scale = lax.rsqrt(total / (peers * width) + EPS)
        for s in range(peers):
            cols = slice(s * width, (s + 1) * width)
            nb[rows, cols] = (xg[s, rows].astype(F32) * scale * gain[:, cols]).astype(BF16)
        return rows

    def blocks(now, query_raw, forget_raw, value_raw):
        for b in range(chunk // BLK):
            inner = slice(b * BLK, (b + 1) * BLK)
            block(
                aligned(now * chunk + b * BLK, BLK),
                query_raw[inner],
                forget_raw[inner],
                value_raw[inner],
            )

    lag = me % 2

    @pl.loop(0, steps + lag)
    def _(step):
        @pl.when(step < steps)
        def _():
            with jax.named_scope("wait_cross"):
                hop(step, cross, cross, csend, crecv).wait_recv()
            hop(step, cross, partner, fsend, frecv).start()

        @pl.when((step >= lag) & (step < steps - 1 + lag))
        def _():
            now = step - lag
            @pl.when(now == 0)
            def _():
                partner_copy(partner).wait_recv()
                surge_copy.wait()
                for j in range(5):
                    weight_copy(j).wait()

            rows = arrive(now)
            blocks(now, *(project(rows, j) for j in range(3)))

            @pl.when(now < steps // 2)
            def _():
                blend(rows, now)

            @pl.when(now == 0)
            def _():
                @pl.when(seq < sp - 1)
                def _():
                    pl.semaphore_wait(ready, sp - 1 - seq)

                @pl.when(seq != start_owner)
                def _():
                    start_hop(seq % ratio).start()

                @pl.when(seq == start_owner)
                def _():
                    start_land[seq % ratio] = start_ref[...]

    def enter(i, g):
        for to in (i,) if i < sp - 2 else (i, i + 1):

            @pl.when(seq != to)
            def _():
                enter_hop(g, i, own, to).start()

            @pl.when(seq == to)
            def _():
                back[own, g] = ent[i, g]

    @pl.when(is_owner)
    def _():
        for r in range(ratio):

            @pl.when(seq != own * ratio + r)
            def _():
                start_hop(r).wait_recv()

        for g in range(groups):
            for t in range(team):
                running = jnp.concatenate(
                    [start_land[r, g * team + t] for r in range(ratio)], axis=0
                )
                carry[g, t] = running
                ent[0, g, t] = running.astype(BF16)
        for g in range(groups):
            enter(0, g)

    final = steps - 1
    rows = arrive(final)
    packing = jax.named_scope("pack")
    packing.__enter__()
    span = team * DK
    row = lax.broadcasted_iota(jnp.int32, (chunk, chunk), 0)
    col = lax.broadcasted_iota(jnp.int32, (chunk, chunk), 1)
    later = (col > row).astype(F32).astype(BF16)
    later = jnp.concatenate([later] * 3, axis=1)
    raw[0], raw[1] = project(rows, 1), project(rows, 2)
    keys = (1.0 - fmin_ref[...]) * jax.nn.sigmoid(-raw[0].astype(F32))
    logs = jnp.log1p(-keys) + surge[rows, :]
    after = jnp.dot(later, split_terms(logs), preferred_element_type=F32)
    total = after[0:1, :] + logs[0:1, :]
    k_all = (keys * jnp.exp(after)).astype(BF16)
    whole_all = jnp.exp(total)
    gone = jnp.exp(run[...] + total)
    for h in range(heads):
        decs[h // team, h % team : h % team + 1, :] = gone[:, h * DK : (h + 1) * DK]

    @pl.when(seq < sp - 2)
    def _():
        for k in range(owners):

            @pl.when(seq != first_owner + k)
            def _():
                decay_hop(seq, first_owner + k).start()

    for g in range(groups):
        cols = slice(g * span, (g + 1) * span)
        value_raw, k_out, whole = raw[1, :, cols], k_all[:, cols], whole_all[:, cols]
        for t in range(team):
            ch = slice(t * DK, (t + 1) * DK)
            state = st[g * team + t] * whole[:, ch] + tn_dot(value_raw[:, ch], k_out[:, ch])
            state = state.T
            for k in range(owners):
                pack[k, g, t] = state[k * piece : (k + 1) * piece].astype(BF16)

        @pl.when(seq < sp - 2)
        def _():
            for k in range(owners):

                @pl.when(seq != first_owner + k)
                def _():
                    state_hop(g, k, seq, first_owner + k).start()

    @pl.when(seq == sp - 2)
    def _():
        pair_decay_hop().start()
        pair_hop().start()

    @pl.when(is_owner & (seq < sp - 2))
    def _():
        land[seq] = pack[own]
        land_decay[seq] = decs[...]

    packing.__exit__(None, None, None)

    def combine(g, low, high):
        with jax.named_scope("wait_states"):
            stage = 0 if low < split else 1
            inside = (seq >= low) & (seq < high)

            def waits(count):
                if g == 0 and count > 0:
                    lines = land_decay.at[pl.ds(0, count)]
                    give(lines, lines, sd.at[0], rd.at[stage], {"sp": seq}).wait_recv()
                if count > 0:
                    parts = land.at[pl.ds(0, count), g]
                    give(parts, parts, s1.at[0], r1.at[g, stage], {"sp": seq}).wait_recv()

            @pl.when(inside)
            def _():
                waits(high - low - 1)

            @pl.when(jnp.logical_not(inside))
            def _():
                waits(high - low)

        lane = lax.broadcasted_iota(jnp.int32, (piece, DK), 1)
        pick = lane == own * piece + lax.broadcasted_iota(jnp.int32, (piece, DK), 0)
        for t in range(team):
            running = carry[g, t]
            for i in range(low, high):
                line = jnp.broadcast_to(land_decay[i, g, t : t + 1, :], (piece, DK))
                decay = jnp.sum(jnp.where(pick, line, 0.0), axis=-1, keepdims=True)
                running = decay * running + land[i, g, t].astype(F32)
                ent[i + 1, g, t] = running.astype(BF16)
            carry[g, t] = running
        for i in outward(low + 1, high):
            enter(i, g)

    gates = jax.named_scope("gates_a")
    gates.__enter__()
    for j in range(5, 7):
        weight_copy(j).wait()
    blocks(final, project(rows, 0), raw[0], raw[1])
    blend(rows, final)

    def prepare(which):
        rows = aligned(which * quarter, quarter)
        post[rows, :] = project(rows, 5)
        gate[rows, :] = project(rows, 6)

    def convolve(which):
        rows = aligned(which * quarter, quarter)
        near = mix[aligned_by(which * quarter, PAD, quarter + PAD), :]
        total = None
        for j in range(CK):
            first = PAD + j - (CK - 1)
            term = near[first : first + quarter, :] * taps_ref[j : j + 1, :].astype(F32)
            total = term if total is None else total + term
        conv = (post[rows, :].astype(F32) * total).astype(BF16)
        acc[rows, :] = jnp.dot(conv, wc[...], preferred_element_type=F32)

    def halo_hop():
        return give(
            mix.at[pl.ds(tokens, PAD)], halo, hs.at[0], hr.at[0], {"sp": (seq + 1) % sp}
        )

    @pl.when(seq < sp - 1)
    def _():
        halo_hop().start()

    prepare(far)
    gates.__exit__(None, None, None)

    @pl.when(is_owner)
    def _():
        for low, high in ((0, split), (split, sp - 2)):
            for g in range(groups):
                combine(g, low, high)

    gates = jax.named_scope("gates_c")
    gates.__enter__()
    prepare(cross)
    @pl.loop(steps // 2, final)
    def _(now):
        blend(aligned(now * chunk, chunk), now)

    mix[0:PAD, :] = jnp.zeros((PAD, width), F32)

    @pl.when(seq > 0)
    def _():
        halo_hop().wait_recv()
        mix[0:PAD, :] = halo[...]

    wc_copy.wait()
    wr_copy.wait()
    convolve(far)
    convolve(cross)
    gates.__exit__(None, None, None)
    def whole_state(pieces_ref, h):
        return jnp.concatenate(
            [pieces_ref[k, h // team, h % team].astype(F32) for k in range(owners)], axis=0
        )

    @pl.when(seq == sp - 1)
    def _():
        pair_decay_hop().wait_recv()
        pair_hop().wait_recv()
        for h in range(heads):
            line = pair_decs[h // team, h % team : h % team + 1, :]
            pair_factor[h] = jnp.broadcast_to(line, (DV, DK)).T

    with jax.named_scope("wait_entering"):
        def entered(count):
            if count > 0:
                parts = back.at[pl.ds(0, count)]
                give(parts, parts, s2.at[0], r2.at[0], {"sp": seq}).wait_recv()

        @pl.when(is_owner)
        def _():
            entered(owners - 1)

        @pl.when(jnp.logical_not(is_owner))
        def _():
            entered(owners)

    @pl.when(seq < sp - 1)
    def _():
        for h in range(heads):
            land_state[h] = whole_state(back, h).astype(BF16)

    @pl.when(seq == sp - 1)
    def _():
        for h in range(heads):
            land_state[h] = (
                pair_factor[h] * whole_state(back, h) + whole_state(pair_land, h)
            ).astype(BF16)

    def mixed(which, s):
        rows = aligned(which * quarter + s * size, size)
        gated = []
        for h in range(heads):
            ch = slice(h * DV, (h + 1) * DV)
            recur = part[rows, ch] + jnp.dot(
                shift[rows, ch], land_state[h], preferred_element_type=F32
            )
            g = gate[rows, ch].astype(F32)
            gated.append(
                (
                    recur * rms_scale(recur) * hgain_ref[...].astype(F32) * (g * jax.nn.sigmoid(g))
                ).astype(BF16)
            )
        rec = jnp.concatenate(gated, axis=1)
        return acc[rows, :] + jnp.dot(rec, wr[...], preferred_element_type=F32)

    def put(which, s):
        rows = aligned(which * quarter + s * size, size)
        acc[rows, :] = mixed(which, s)

    def partner_hop(i):
        return give(pbuf.at[i], prcv.at[i], ps.at[0], pr.at[i], {"tp": partner})

    def cross_hop(i):
        return give(cbuf.at[i], crcv.at[i], cs.at[0], cr.at[i], {"tp": cross})

    def share(which, s, slot):
        pbuf[slot] = mixed(which, s).astype(BF16)
        partner_hop(slot).start()

    def forward(s):
        partner_hop(s).wait_recv()
        rows = aligned(cross * quarter + s * size, size)
        cbuf[s] = (acc[rows, :] + prcv[s].astype(F32)).astype(BF16)
        cross_hop(s).start()

    sums = jax.named_scope("sums")
    sums.__enter__()

    @pl.loop(0, pieces + 1)
    def _(s):
        @pl.when(s < pieces)
        def _():
            share(far, s, s)

        @pl.when(s > 0)
        def _():
            forward(s - 1)

        @pl.when(s < pieces)
        def _():
            put(cross, s)

    prepare(partner)
    convolve(partner)
    prepare(me)
    convolve(me)

    @pl.loop(0, pieces)
    def _(s):
        share(partner, s, pieces + s)
        put(me, s)

    sums.__exit__(None, None, None)
    sent(me, cross, csend, crecv)
    sent(me, partner, psend, precv)
    sent(cross, partner, fsend, frecv)

    def states_sent(count):
        if count > 0:
            parts, lines = pack.at[pl.ds(0, count)], land_decay.at[pl.ds(0, count)]
            give(lines, lines, sd.at[0], rd.at[0], {"sp": seq}).wait_send()
            give(parts, parts, s1.at[0], r1.at[0, 0], {"sp": seq}).wait_send()

    @pl.when((seq < sp - 2) & is_owner)
    def _():
        states_sent(owners - 1)

    @pl.when((seq < sp - 2) & jnp.logical_not(is_owner))
    def _():
        states_sent(owners)

    @pl.when(seq == sp - 2)
    def _():
        pair_decay_hop().wait_send()
        pair_hop().wait_send()

    @pl.when(is_owner)
    def _():
        give(ent, ent, s2.at[0], r2.at[0], {"sp": seq}).wait_send()

    @pl.when(seq != start_owner)
    def _():
        start_hop(seq % ratio).wait_send()

    @pl.when(seq < sp - 1)
    def _():
        halo_hop().wait_send()

    give(pbuf, prcv, ps.at[0], pr.at[0], {"tp": partner}).wait_send()
    last = jax.named_scope("last")
    last.__enter__()
    ogain = row_of(ogain_ref)

    @pl.loop(0, pieces)
    def _(s):
        partner_hop(pieces + s).wait_recv()
        cross_hop(s).wait_recv()
        rows = aligned(me * quarter + s * size, size)
        total = acc[rows, :] + prcv[pieces + s].astype(F32) + crcv[s].astype(F32)
        out_ref[aligned(s * size, size), :] = (total * rms_scale(total) * ogain).astype(BF16)

    last.__exit__(None, None, None)
    with jax.named_scope("sends"):
        give(cbuf, crcv, cs.at[0], cr.at[0], {"tp": cross}).wait_send()


def shards(
    layer_input,
    input_norm_gain,
    query_weight,
    forget_weight,
    value_matrix,
    output_gate_weight,
    after_gate_weight,
    before_gate_weight,
    convolution_input_weight,
    forget_minimum,
    surge_log_decay,
    convolution_kernel,
    head_norm_gain,
    starting_state,
    recurrence_output_weight,
    convolution_output_weight,
    output_norm_gain,
):
    sp, tp = lax.axis_size("sp"), lax.axis_size("tp")
    tokens, width = layer_input.shape
    wide = recurrence_output_weight.shape[1]
    depth, cols = query_weight.shape
    heads = cols // DV
    chunk = 128 if tokens % 128 == 0 else BLK
    steps = tokens // chunk
    quarter = tokens // tp
    pieces = 4 if quarter % 64 == 0 else 2
    size = quarter // pieces
    _, ratio = owner_place(sp)
    owners = sp // ratio
    groups = 2 if heads % 2 == 0 else 1
    team = heads // groups
    share = (groups, team, DK // owners, DV)
    vmem = pl.BlockSpec(memory_space=pltpu.VMEM)
    hbm = pl.BlockSpec(memory_space=pltpu.HBM)
    dma = pltpu.SemaphoreType.DMA
    return pl.pallas_call(
        functools.partial(layer_kernel, heads, chunk, pieces),
        out_shape=pltpu.VMEM((quarter, wide), BF16),
        in_specs=[hbm] * 17,
        out_specs=vmem,
        scratch_shapes=[
            pltpu.VMEM((7, depth, cols), BF16),
            pltpu.VMEM((tp, tokens, width), BF16),
            pltpu.VMEM((tokens, depth), BF16),
            pltpu.VMEM((tokens, cols), F32),
            pltpu.VMEM((tokens, cols), F32),
            pltpu.VMEM((tokens, cols), BF16),
            pltpu.VMEM((heads, DV, DK), F32),
            pltpu.VMEM((1, cols), F32),
            pltpu.VMEM((2, chunk, cols), BF16),
            pltpu.VMEM(share, F32),
            pltpu.VMEM((owners,) + share, BF16),
            pltpu.VMEM((groups, team, DK), F32),
            pltpu.VMEM((heads, DK, DV), F32),
            pltpu.VMEM((ratio,) + starting_state.shape, F32),
            pltpu.VMEM((owners,) + share, BF16),
            pltpu.VMEM((groups, team, DK), F32),
            pltpu.VMEM((sp,) + share, BF16),
            pltpu.VMEM((sp, groups, team, DK), F32),
            pltpu.VMEM((sp - 1,) + share, BF16),
            pltpu.VMEM((owners,) + share, BF16),
            pltpu.VMEM((tokens, cols), BF16),
            pltpu.VMEM((tokens, cols), BF16),
            pltpu.VMEM((tokens + PAD, cols), F32),
            pltpu.VMEM((PAD, cols), F32),
            pltpu.VMEM((cols, wide), BF16),
            pltpu.VMEM((cols, wide), BF16),
            pltpu.VMEM((tokens, wide), F32),
            pltpu.VMEM((2 * pieces, size, wide), BF16),
            pltpu.VMEM((2 * pieces, size, wide), BF16),
            pltpu.VMEM((pieces, size, wide), BF16),
            pltpu.VMEM((pieces, size, wide), BF16),
            pltpu.VMEM((heads, DK, DV), BF16),
            pltpu.VMEM((depth // LANES, LANES), BF16),
            pltpu.VMEM((1, cols), F32),
            pltpu.VMEM((CK, cols), BF16),
            pltpu.VMEM((1, DV), BF16),
            pltpu.VMEM(starting_state.shape, F32),
            pltpu.VMEM((wide // LANES, LANES), BF16),
            dma((17,)),
        ]
        + [dma((1,)), dma((steps,)), dma((1,)), dma((1,)), dma((1,)), dma((steps,))]
        + [dma((1,)), dma((groups, 2)), dma((1,)), dma((2,)), dma((1,)), dma((1,))]
        + [dma((1,))] * 2
        + [dma((1,)), dma((2 * pieces,)), dma((1,)), dma((pieces,))]
        + [pltpu.SemaphoreType.REGULAR]
        + [dma((1,)), dma((ratio,)), dma((2,)), dma((2,))],
        compiler_params=pltpu.CompilerParams(collective_id=0, has_side_effects=True, vmem_limit_bytes=56 * 1024 * 1024),
        name="layer",
    )(
        layer_input,
        input_norm_gain.reshape(-1, LANES),
        query_weight,
        forget_weight,
        value_matrix,
        before_gate_weight,
        convolution_input_weight,
        after_gate_weight,
        output_gate_weight,
        surge_log_decay,
        forget_minimum[None, :],
        convolution_kernel,
        head_norm_gain[None, :],
        starting_state,
        recurrence_output_weight,
        convolution_output_weight,
        output_norm_gain.reshape(-1, LANES),
    )


def solution(mesh):
    return jax.shard_map(
        shards,
        mesh=mesh,
        in_specs=(
            P("sp", "tp"),
            P(),
            P(None, "tp"),
            P(None, "tp"),
            P(None, "tp"),
            P(None, "tp"),
            P(None, "tp"),
            P(None, "tp"),
            P(None, "tp"),
            P("tp"),
            P("sp", "tp"),
            P(None, "tp"),
            P(),
            P("tp", "sp", None),
            P("tp", None),
            P("tp", None),
            P(),
        ),
        out_specs=P(("sp", "tp"), None),
        check_vma=False,
    )
```

```python
import functools

import jax
import jax.numpy as jnp
from jax import lax
from jax.experimental import pallas as pl
from jax.experimental.pallas import tpu as pltpu
from jax.sharding import PartitionSpec as P

DK = 128
DV = 128
CK = 3
BLK = 64
LANES = 128
PAD = 8


EPS = 1e-06
F32 = jnp.float32
BF16 = jnp.bfloat16
MESH = pl.DeviceIdType.MESH


def rms_scale(value_rows):
    return lax.rsqrt(jnp.mean(value_rows * value_rows, axis=-1, keepdims=True) + EPS)


def nt_dot(a, b):
    return lax.dot_general(a, b, (((1,), (1,)), ((), ())), preferred_element_type=F32)


def tn_dot(a, b):
    return lax.dot_general(a, b, (((0,), (0,)), ((), ())), preferred_element_type=F32)


def split_terms(logs):
    high = logs.astype(BF16)
    rest = logs - high.astype(F32)
    next_term = rest.astype(BF16)
    low = (rest - next_term.astype(F32)).astype(BF16)
    return jnp.concatenate([high, next_term, low], axis=0)


def tp_places():
    me = lax.axis_index("tp")
    pair, core = me // 2, me % 2
    partner = 2 * pair + (1 - core)
    cross = 2 * (1 - pair) + core
    far = 2 * (1 - pair) + (1 - core)
    return me, partner, cross, far


def owner_place(sp):
    owners = max(1, sp // 2)
    return (sp - owners) // 2, sp // owners


def outward(low, high):
    order = []
    while low <= high:
        order += [low, high] if low < high else [low]
        low, high = low + 1, high - 1
    return order


def aligned(start, size):
    return pl.ds(pl.multiple_of(start, size), size)


def aligned_by(start, step, size):
    return pl.ds(pl.multiple_of(start, step), size)


def row_of(ref):
    lines = ref[...].astype(F32)
    return jnp.concatenate([lines[i : i + 1, :] for i in range(lines.shape[0])], axis=1)


def layer_kernel(
    heads,
    chunk,
    pieces,
    x_hbm,
    gain_hbm,
    wq_hbm,
    wf_hbm,
    wv_hbm,
    wpre_hbm,
    wconv_hbm,
    wpost_hbm,
    wout_hbm,
    surge_hbm,
    fmin_hbm,
    taps_hbm,
    hgain_hbm,
    start_hbm,
    wr_hbm,
    wc_hbm,
    ogain_hbm,
    out_ref,
    wbuf,
    xg,
    nb,
    surge,
    part,
    shift,
    st,
    run,
    raw,
    carry,
    pair_land,
    pair_decs,
    pair_factor,
    start_land,
    pack,
    decs,
    land,
    land_decay,
    ent,
    back,
    gate,
    post,
    mix,
    halo,
    wr,
    wc,
    acc,
    pbuf,
    prcv,
    cbuf,
    crcv,
    land_state,
    gain_ref,
    fmin_ref,
    taps_ref,
    hgain_ref,
    start_ref,
    ogain_ref,
    lsem,
    csend,
    crecv,
    psend,
    precv,
    fsend,
    frecv,
    s1,
    r1,
    sd,
    rd,
    s2,
    r2,
    hs,
    hr,
    ps,
    pr,
    cs,
    cr,
    ready,
    ss,
    sr,
    qs,
    qr,
):
    peers, tokens, width = xg.shape
    groups, team = decs.shape[:2]
    owners, piece = back.shape[0], back.shape[3]
    first_owner, ratio = owner_place(lax.axis_size("sp"))
    steps = tokens // chunk
    sp = lax.axis_size("sp")
    seq = lax.axis_index("sp")
    quarter = tokens // peers
    size = quarter // pieces
    me, partner, cross, far = tp_places()
    sources = (wq_hbm, wf_hbm, wv_hbm, wpre_hbm, wconv_hbm, wpost_hbm, wout_hbm)

    x_copy = pltpu.make_async_copy(x_hbm, xg.at[me], lsem.at[0])
    surge_copy = pltpu.make_async_copy(surge_hbm, surge, lsem.at[1])
    wr_copy = pltpu.make_async_copy(wr_hbm, wr, lsem.at[2])
    wc_copy = pltpu.make_async_copy(wc_hbm, wc, lsem.at[3])

    def weight_copy(j):
        return pltpu.make_async_copy(sources[j], wbuf.at[j], lsem.at[4 + j])

    x_copy.start()
    smalls = (
        (gain_hbm, gain_ref),
        (fmin_hbm, fmin_ref),
        (taps_hbm, taps_ref),
        (hgain_hbm, hgain_ref),
        (start_hbm, start_ref),
        (ogain_hbm, ogain_ref),
    )
    small_copies = [
        pltpu.make_async_copy(src, dst, lsem.at[11 + i]) for i, (src, dst) in enumerate(smalls)
    ]
    barrier = pltpu.get_barrier_semaphore()
    for other in (partner, cross):
        pl.semaphore_signal(barrier, inc=1, device_id={"tp": other}, device_id_type=MESH)
    for off in range(1, sp):
        to = (seq + off) % sp

        @pl.when(to > seq)
        def _():
            pl.semaphore_signal(barrier, inc=1, device_id={"sp": to}, device_id_type=MESH)

    for copy in small_copies:
        copy.start()
    for j in range(3):
        weight_copy(j).start()
    surge_copy.start()
    with jax.named_scope("entry"):
        x_copy.wait()
        pl.semaphore_wait(barrier, 2 + seq)

    def give(src, dst, send, recv, to):
        return pltpu.make_async_remote_copy(
            src_ref=src,
            dst_ref=dst,
            send_sem=send,
            recv_sem=recv,
            device_id=to,
            device_id_type=MESH,
        )

    def hop(step, slot, to, send, recv):
        rows = aligned(step * chunk, chunk)
        return give(xg.at[slot, rows], xg.at[slot, rows], send.at[0], recv.at[step], {"tp": to})

    def sent(slot, to, send, recv):
        give(xg.at[slot], xg.at[slot], send.at[0], recv.at[0], {"tp": to}).wait_send()

    def partner_copy(slot):
        return give(xg.at[slot], xg.at[slot], psend.at[0], precv.at[0], {"tp": partner})

    for step in range(steps):
        hop(step, me, cross, csend, crecv).start()
    partner_copy(me).start()
    for j in range(3, 7):
        weight_copy(j).start()
    wc_copy.start()
    wr_copy.start()

    own = jnp.clip(seq - first_owner, 0, owners - 1)
    is_owner = (seq >= first_owner) & (seq < first_owner + owners)
    start_owner = first_owner + seq // ratio

    split = sp // 4

    def stage_of(slot):
        return jnp.where(slot < split, 0, 1)

    def state_hop(g, k, slot, to):
        return give(
            pack.at[k, g], land.at[slot, g], s1.at[0], r1.at[g, stage_of(slot)], {"sp": to}
        )

    def decay_hop(slot, to):
        return give(decs, land_decay.at[slot], sd.at[0], rd.at[stage_of(slot)], {"sp": to})

    def enter_hop(g, i, slot, to):
        return give(ent.at[i, g], back.at[slot, g], s2.at[0], r2.at[0], {"sp": to})

    def pair_hop():
        return give(pack, pair_land, qs.at[0], qr.at[0], {"sp": (seq + 1) % sp})

    def pair_decay_hop():
        return give(decs, pair_decs, qs.at[1], qr.at[1], {"sp": (seq + 1) % sp})

    def start_hop(slot):
        return give(
            start_ref, start_land.at[slot], ss.at[0], sr.at[slot], {"sp": start_owner}
        )

    for off in range(1, sp):
        to = (seq + off) % sp

        @pl.when(to < seq)
        def _():
            pl.semaphore_signal(ready, inc=1, device_id={"sp": to}, device_id_type=MESH)

    for copy in small_copies:
        copy.wait()

    st[...] = jnp.zeros_like(st)
    run[...] = jnp.zeros_like(run)
    gain = row_of(gain_ref)
    row = lax.broadcasted_iota(jnp.int32, (BLK, BLK), 0)
    col = lax.broadcasted_iota(jnp.int32, (BLK, BLK), 1)
    causal = col <= row
    middle = (causal.astype(F32) - (col < BLK // 2).astype(F32)).astype(BF16)
    middle = jnp.concatenate([middle] * 3, axis=1)

    def block(rows, query_raw, forget_raw, values):
        forget = forget_raw.astype(F32)
        keys = (1.0 - fmin_ref[...]) * jax.nn.sigmoid(-forget)
        logs = jnp.log1p(-keys) + surge[rows, :]
        rel = jnp.dot(middle, split_terms(logs), preferred_element_type=F32)
        mid = logs[0:1, :] - rel[0:1, :]
        tail = rel[BLK - 1 : BLK, :]
        raw = query_raw.astype(F32)
        queries = raw * jax.nn.sigmoid(raw) * DK ** (-0.5)
        q_mid = queries * jnp.exp(rel)
        k_mid = keys * jnp.exp(-rel)
        q_in = q_mid * jnp.exp(mid)
        k_out = (k_mid * jnp.exp(tail)).astype(BF16)
        whole = jnp.exp(mid + tail)
        shift[rows, :] = (q_in * jnp.exp(run[...])).astype(BF16)
        run[...] = run[...] + mid + tail
        q_mid = q_mid.astype(BF16)
        k_mid = k_mid.astype(BF16)
        q_in = q_in.astype(BF16)
        for h in range(heads):
            ch = slice(h * DK, (h + 1) * DK)
            scores = jnp.where(causal, nt_dot(q_mid[:, ch], k_mid[:, ch]), 0.0).astype(BF16)
            before = st[h]
            part[rows, ch] = jnp.dot(
                scores, values[:, ch], preferred_element_type=F32
            ) + nt_dot(q_in[:, ch], before.astype(BF16))
            st[h] = before * whole[:, ch] + tn_dot(values[:, ch], k_out[:, ch])

    def project(rows, j):
        return jnp.dot(nb[rows, :], wbuf[j], preferred_element_type=F32).astype(BF16)

    def blend(rows, now):
        mix[aligned_by(PAD + now * chunk, PAD, chunk), :] = project(rows, 3).astype(
            F32
        ) * project(rows, 4).astype(F32)

    def arrive(now):
        with jax.named_scope("wait_forward"):
            hop(now, far, partner, fsend, frecv).wait_recv()
        rows = aligned(now * chunk, chunk)
        squares = jnp.zeros((chunk, width), F32)
        for s in range(peers):
            part_x = xg[s, rows].astype(F32)
            squares = squares + part_x * part_x
        total = jnp.sum(squares, axis=-1, keepdims=True)
        scale = lax.rsqrt(total / (peers * width) + EPS)
        for s in range(peers):
            cols = slice(s * width, (s + 1) * width)
            nb[rows, cols] = (xg[s, rows].astype(F32) * scale * gain[:, cols]).astype(BF16)
        return rows

    def blocks(now, query_raw, forget_raw, value_raw):
        for b in range(chunk // BLK):
            inner = slice(b * BLK, (b + 1) * BLK)
            block(
                aligned(now * chunk + b * BLK, BLK),
                query_raw[inner],
                forget_raw[inner],
                value_raw[inner],
            )

    lag = me % 2

    @pl.loop(0, steps + lag)
    def _(step):
        @pl.when(step < steps)
        def _():
            with jax.named_scope("wait_cross"):
                hop(step, cross, cross, csend, crecv).wait_recv()
            hop(step, cross, partner, fsend, frecv).start()

        @pl.when((step >= lag) & (step < steps - 1 + lag))
        def _():
            now = step - lag
            @pl.when(now == 0)
            def _():
                partner_copy(partner).wait_recv()
                surge_copy.wait()
                for j in range(5):
                    weight_copy(j).wait()

            rows = arrive(now)
            blocks(now, *(project(rows, j) for j in range(3)))

            @pl.when(now < steps - 2)
            def _():
                blend(rows, now)

            @pl.when(now == 0)
            def _():
                @pl.when(seq < sp - 1)
                def _():
                    pl.semaphore_wait(ready, sp - 1 - seq)

                @pl.when(seq != start_owner)
                def _():
                    start_hop(seq % ratio).start()

                @pl.when(seq == start_owner)
                def _():
                    start_land[seq % ratio] = start_ref[...]

    def enter(i, g):
        for to in (i,) if i < sp - 2 else (i, i + 1):

            @pl.when(seq != to)
            def _():
                enter_hop(g, i, own, to).start()

            @pl.when(seq == to)
            def _():
                back[own, g] = ent[i, g]

    @pl.when(is_owner)
    def _():
        for r in range(ratio):

            @pl.when(seq != own * ratio + r)
            def _():
                start_hop(r).wait_recv()

        for g in range(groups):
            for t in range(team):
                running = jnp.concatenate(
                    [start_land[r, g * team + t] for r in range(ratio)], axis=0
                )
                carry[g, t] = running
                ent[0, g, t] = running.astype(BF16)
        for g in range(groups):
            enter(0, g)

    final = steps - 1
    rows = arrive(final)
    packing = jax.named_scope("pack")
    packing.__enter__()
    span = team * DK
    row = lax.broadcasted_iota(jnp.int32, (chunk, chunk), 0)
    col = lax.broadcasted_iota(jnp.int32, (chunk, chunk), 1)
    later = (col > row).astype(F32).astype(BF16)
    later = jnp.concatenate([later] * 3, axis=1)
    raw[0], raw[1] = project(rows, 1), project(rows, 2)
    keys = (1.0 - fmin_ref[...]) * jax.nn.sigmoid(-raw[0].astype(F32))
    logs = jnp.log1p(-keys) + surge[rows, :]
    after = jnp.dot(later, split_terms(logs), preferred_element_type=F32)
    total = after[0:1, :] + logs[0:1, :]
    k_all = (keys * jnp.exp(after)).astype(BF16)
    whole_all = jnp.exp(total)
    gone = jnp.exp(run[...] + total)
    for h in range(heads):
        decs[h // team, h % team : h % team + 1, :] = gone[:, h * DK : (h + 1) * DK]

    @pl.when(seq < sp - 2)
    def _():
        for k in range(owners):

            @pl.when(seq != first_owner + k)
            def _():
                decay_hop(seq, first_owner + k).start()

    for g in range(groups):
        cols = slice(g * span, (g + 1) * span)
        value_raw, k_out, whole = raw[1, :, cols], k_all[:, cols], whole_all[:, cols]
        for t in range(team):
            ch = slice(t * DK, (t + 1) * DK)
            state = st[g * team + t] * whole[:, ch] + tn_dot(value_raw[:, ch], k_out[:, ch])
            state = state.T
            for k in range(owners):
                pack[k, g, t] = state[k * piece : (k + 1) * piece].astype(BF16)

        @pl.when(seq < sp - 2)
        def _():
            for k in range(owners):

                @pl.when(seq != first_owner + k)
                def _():
                    state_hop(g, k, seq, first_owner + k).start()

    @pl.when(seq == sp - 2)
    def _():
        pair_decay_hop().start()
        pair_hop().start()

    @pl.when(is_owner & (seq < sp - 2))
    def _():
        land[seq] = pack[own]
        land_decay[seq] = decs[...]

    packing.__exit__(None, None, None)

    def combine(g, low, high):
        with jax.named_scope("wait_states"):
            stage = 0 if low < split else 1
            inside = (seq >= low) & (seq < high)

            def waits(count):
                if g == 0 and count > 0:
                    lines = land_decay.at[pl.ds(0, count)]
                    give(lines, lines, sd.at[0], rd.at[stage], {"sp": seq}).wait_recv()
                if count > 0:
                    parts = land.at[pl.ds(0, count), g]
                    give(parts, parts, s1.at[0], r1.at[g, stage], {"sp": seq}).wait_recv()

            @pl.when(inside)
            def _():
                waits(high - low - 1)

            @pl.when(jnp.logical_not(inside))
            def _():
                waits(high - low)

        lane = lax.broadcasted_iota(jnp.int32, (piece, DK), 1)
        pick = lane == own * piece + lax.broadcasted_iota(jnp.int32, (piece, DK), 0)
        for t in range(team):
            running = carry[g, t]
            for i in range(low, high):
                line = jnp.broadcast_to(land_decay[i, g, t : t + 1, :], (piece, DK))
                decay = jnp.sum(jnp.where(pick, line, 0.0), axis=-1, keepdims=True)
                running = decay * running + land[i, g, t].astype(F32)
                ent[i + 1, g, t] = running.astype(BF16)
            carry[g, t] = running
        for i in outward(low + 1, high):
            enter(i, g)

    gates = jax.named_scope("gates_a")
    gates.__enter__()
    for j in range(5, 7):
        weight_copy(j).wait()
    blocks(final, project(rows, 0), raw[0], raw[1])
    blend(rows, final)

    def prepare(which):
        rows = aligned(which * quarter, quarter)
        post[rows, :] = project(rows, 5)
        gate[rows, :] = project(rows, 6)

    def convolve(which):
        rows = aligned(which * quarter, quarter)
        near = mix[aligned_by(which * quarter, PAD, quarter + PAD), :]
        total = None
        for j in range(CK):
            first = PAD + j - (CK - 1)
            term = near[first : first + quarter, :] * taps_ref[j : j + 1, :].astype(F32)
            total = term if total is None else total + term
        conv = (post[rows, :].astype(F32) * total).astype(BF16)
        acc[rows, :] = jnp.dot(conv, wc[...], preferred_element_type=F32)

    def halo_hop():
        return give(
            mix.at[pl.ds(tokens, PAD)], halo, hs.at[0], hr.at[0], {"sp": (seq + 1) % sp}
        )

    @pl.when(seq < sp - 1)
    def _():
        halo_hop().start()

    prepare(far)
    gates.__exit__(None, None, None)

    @pl.when(is_owner)
    def _():
        for low, high in ((0, split), (split, sp - 2)):
            for g in range(groups):
                combine(g, low, high)

    gates = jax.named_scope("gates_c")
    gates.__enter__()
    prepare(cross)
    @pl.loop(steps - 2, final)
    def _(now):
        blend(aligned(now * chunk, chunk), now)

    mix[0:PAD, :] = jnp.zeros((PAD, width), F32)

    @pl.when(seq > 0)
    def _():
        halo_hop().wait_recv()
        mix[0:PAD, :] = halo[...]

    wc_copy.wait()
    wr_copy.wait()
    convolve(far)
    convolve(cross)
    gates.__exit__(None, None, None)
    def whole_state(pieces_ref, h):
        return jnp.concatenate(
            [pieces_ref[k, h // team, h % team].astype(F32) for k in range(owners)], axis=0
        )

    @pl.when(seq == sp - 1)
    def _():
        pair_decay_hop().wait_recv()
        pair_hop().wait_recv()
        for h in range(heads):
            line = pair_decs[h // team, h % team : h % team + 1, :]
            pair_factor[h] = jnp.broadcast_to(line, (DV, DK)).T

    with jax.named_scope("wait_entering"):
        def entered(count):
            if count > 0:
                parts = back.at[pl.ds(0, count)]
                give(parts, parts, s2.at[0], r2.at[0], {"sp": seq}).wait_recv()

        @pl.when(is_owner)
        def _():
            entered(owners - 1)

        @pl.when(jnp.logical_not(is_owner))
        def _():
            entered(owners)

    @pl.when(seq < sp - 1)
    def _():
        for h in range(heads):
            if piece % 16 == 0:
                for k in range(owners):
                    land_state[h, k * piece : (k + 1) * piece, :] = back[k, h // team, h % team]
            else:
                land_state[h] = whole_state(back, h).astype(BF16)

    @pl.when(seq == sp - 1)
    def _():
        for h in range(heads):
            land_state[h] = (
                pair_factor[h] * whole_state(back, h) + whole_state(pair_land, h)
            ).astype(BF16)

    def mixed(which, s):
        rows = aligned(which * quarter + s * size, size)
        gated = []
        for h in range(heads):
            ch = slice(h * DV, (h + 1) * DV)
            recur = part[rows, ch] + jnp.dot(
                shift[rows, ch], land_state[h], preferred_element_type=F32
            )
            g = gate[rows, ch].astype(F32)
            gated.append(
                (
                    recur * rms_scale(recur) * hgain_ref[...].astype(F32) * (g * jax.nn.sigmoid(g))
                ).astype(BF16)
            )
        rec = jnp.concatenate(gated, axis=1)
        return acc[rows, :] + jnp.dot(rec, wr[...], preferred_element_type=F32)

    def put(which, s):
        rows = aligned(which * quarter + s * size, size)
        acc[rows, :] = mixed(which, s)

    def partner_hop(i):
        return give(pbuf.at[i], prcv.at[i], ps.at[0], pr.at[i], {"tp": partner})

    def cross_hop(i):
        return give(cbuf.at[i], crcv.at[i], cs.at[0], cr.at[i], {"tp": cross})

    def share(which, s, slot):
        pbuf[slot] = mixed(which, s).astype(BF16)
        partner_hop(slot).start()

    def forward(s):
        partner_hop(s).wait_recv()
        rows = aligned(cross * quarter + s * size, size)
        cbuf[s] = (acc[rows, :] + prcv[s].astype(F32)).astype(BF16)
        cross_hop(s).start()

    sums = jax.named_scope("sums")
    sums.__enter__()

    @pl.loop(0, pieces + 1)
    def _(s):
        @pl.when(s < pieces)
        def _():
            share(far, s, s)

        @pl.when(s > 0)
        def _():
            forward(s - 1)

        @pl.when(s < pieces)
        def _():
            put(cross, s)

    prepare(partner)
    convolve(partner)
    prepare(me)
    convolve(me)

    @pl.loop(0, pieces)
    def _(s):
        share(partner, s, pieces + s)
        put(me, s)

    sums.__exit__(None, None, None)
    sent(me, cross, csend, crecv)
    sent(me, partner, psend, precv)
    sent(cross, partner, fsend, frecv)

    def states_sent(count):
        if count > 0:
            parts, lines = pack.at[pl.ds(0, count)], land_decay.at[pl.ds(0, count)]
            give(lines, lines, sd.at[0], rd.at[0], {"sp": seq}).wait_send()
            give(parts, parts, s1.at[0], r1.at[0, 0], {"sp": seq}).wait_send()

    @pl.when((seq < sp - 2) & is_owner)
    def _():
        states_sent(owners - 1)

    @pl.when((seq < sp - 2) & jnp.logical_not(is_owner))
    def _():
        states_sent(owners)

    @pl.when(seq == sp - 2)
    def _():
        pair_decay_hop().wait_send()
        pair_hop().wait_send()

    @pl.when(is_owner)
    def _():
        give(ent, ent, s2.at[0], r2.at[0], {"sp": seq}).wait_send()

    @pl.when(seq != start_owner)
    def _():
        start_hop(seq % ratio).wait_send()

    @pl.when(seq < sp - 1)
    def _():
        halo_hop().wait_send()

    give(pbuf, prcv, ps.at[0], pr.at[0], {"tp": partner}).wait_send()
    last = jax.named_scope("last")
    last.__enter__()
    ogain = row_of(ogain_ref)

    @pl.loop(0, pieces)
    def _(s):
        partner_hop(pieces + s).wait_recv()
        cross_hop(s).wait_recv()
        rows = aligned(me * quarter + s * size, size)
        total = acc[rows, :] + prcv[pieces + s].astype(F32) + crcv[s].astype(F32)
        out_ref[aligned(s * size, size), :] = (total * rms_scale(total) * ogain).astype(BF16)

    last.__exit__(None, None, None)
    with jax.named_scope("sends"):
        give(cbuf, crcv, cs.at[0], cr.at[0], {"tp": cross}).wait_send()


def shards(
    layer_input,
    input_norm_gain,
    query_weight,
    forget_weight,
    value_matrix,
    output_gate_weight,
    after_gate_weight,
    before_gate_weight,
    convolution_input_weight,
    forget_minimum,
    surge_log_decay,
    convolution_kernel,
    head_norm_gain,
    starting_state,
    recurrence_output_weight,
    convolution_output_weight,
    output_norm_gain,
):
    sp, tp = lax.axis_size("sp"), lax.axis_size("tp")
    tokens, width = layer_input.shape
    wide = recurrence_output_weight.shape[1]
    depth, cols = query_weight.shape
    heads = cols // DV
    chunk = 128 if tokens % 128 == 0 else BLK
    steps = tokens // chunk
    quarter = tokens // tp
    pieces = 4 if quarter % 64 == 0 else 2
    size = quarter // pieces
    _, ratio = owner_place(sp)
    owners = sp // ratio
    groups = 2 if heads % 2 == 0 else 1
    team = heads // groups
    share = (groups, team, DK // owners, DV)
    vmem = pl.BlockSpec(memory_space=pltpu.VMEM)
    hbm = pl.BlockSpec(memory_space=pltpu.HBM)
    dma = pltpu.SemaphoreType.DMA
    return pl.pallas_call(
        functools.partial(layer_kernel, heads, chunk, pieces),
        out_shape=pltpu.VMEM((quarter, wide), BF16),
        in_specs=[hbm] * 17,
        out_specs=vmem,
        scratch_shapes=[
            pltpu.VMEM((7, depth, cols), BF16),
            pltpu.VMEM((tp, tokens, width), BF16),
            pltpu.VMEM((tokens, depth), BF16),
            pltpu.VMEM((tokens, cols), F32),
            pltpu.VMEM((tokens, cols), F32),
            pltpu.VMEM((tokens, cols), BF16),
            pltpu.VMEM((heads, DV, DK), F32),
            pltpu.VMEM((1, cols), F32),
            pltpu.VMEM((2, chunk, cols), BF16),
            pltpu.VMEM(share, F32),
            pltpu.VMEM((owners,) + share, BF16),
            pltpu.VMEM((groups, team, DK), F32),
            pltpu.VMEM((heads, DK, DV), F32),
            pltpu.VMEM((ratio,) + starting_state.shape, F32),
            pltpu.VMEM((owners,) + share, BF16),
            pltpu.VMEM((groups, team, DK), F32),
            pltpu.VMEM((sp,) + share, BF16),
            pltpu.VMEM((sp, groups, team, DK), F32),
            pltpu.VMEM((sp - 1,) + share, BF16),
            pltpu.VMEM((owners,) + share, BF16),
            pltpu.VMEM((tokens, cols), BF16),
            pltpu.VMEM((tokens, cols), BF16),
            pltpu.VMEM((tokens + PAD, cols), F32),
            pltpu.VMEM((PAD, cols), F32),
            pltpu.VMEM((cols, wide), BF16),
            pltpu.VMEM((cols, wide), BF16),
            pltpu.VMEM((tokens, wide), F32),
            pltpu.VMEM((2 * pieces, size, wide), BF16),
            pltpu.VMEM((2 * pieces, size, wide), BF16),
            pltpu.VMEM((pieces, size, wide), BF16),
            pltpu.VMEM((pieces, size, wide), BF16),
            pltpu.VMEM((heads, DK, DV), BF16),
            pltpu.VMEM((depth // LANES, LANES), BF16),
            pltpu.VMEM((1, cols), F32),
            pltpu.VMEM((CK, cols), BF16),
            pltpu.VMEM((1, DV), BF16),
            pltpu.VMEM(starting_state.shape, F32),
            pltpu.VMEM((wide // LANES, LANES), BF16),
            dma((17,)),
        ]
        + [dma((1,)), dma((steps,)), dma((1,)), dma((1,)), dma((1,)), dma((steps,))]
        + [dma((1,)), dma((groups, 2)), dma((1,)), dma((2,)), dma((1,)), dma((1,))]
        + [dma((1,))] * 2
        + [dma((1,)), dma((2 * pieces,)), dma((1,)), dma((pieces,))]
        + [pltpu.SemaphoreType.REGULAR]
        + [dma((1,)), dma((ratio,)), dma((2,)), dma((2,))],
        compiler_params=pltpu.CompilerParams(collective_id=0, has_side_effects=True, vmem_limit_bytes=56 * 1024 * 1024),
        name="layer",
    )(
        layer_input,
        input_norm_gain.reshape(-1, LANES),
        query_weight,
        forget_weight,
        value_matrix,
        before_gate_weight,
        convolution_input_weight,
        after_gate_weight,
        output_gate_weight,
        surge_log_decay,
        forget_minimum[None, :],
        convolution_kernel,
        head_norm_gain[None, :],
        starting_state,
        recurrence_output_weight,
        convolution_output_weight,
        output_norm_gain.reshape(-1, LANES),
    )


def solution(mesh):
    return jax.shard_map(
        shards,
        mesh=mesh,
        in_specs=(
            P("sp", "tp"),
            P(),
            P(None, "tp"),
            P(None, "tp"),
            P(None, "tp"),
            P(None, "tp"),
            P(None, "tp"),
            P(None, "tp"),
            P(None, "tp"),
            P("tp"),
            P("sp", "tp"),
            P(None, "tp"),
            P(),
            P("tp", "sp", None),
            P("tp", None),
            P("tp", None),
            P(),
        ),
        out_specs=P(("sp", "tp"), None),
        check_vma=False,
    )
```
